512 devices in a mesh: ep: 32 (over z, x), tp: 16 (over y, core).
Axes of the slice: x: 4, y: 8, z: 8, core: 2. Of those that a mesh axis runs over, the one named last changes fastest.
Arguments:
- tokens_a: bfloat16 [4096, 2048], P('ep'), may hold values from -6 to 6
- gain_a: float32 [2048], replicated, may hold values from 0.1 to 1.9
- value_w: bfloat16 [2048, 2048], P(None, 'tp'), may hold values from -0.125 to 0.125
- gate_w: bfloat16 [2048, 2048], P(None, 'tp'), may hold values from -0.125 to 0.125
- kernel: float32 [31, 2048], P(None, 'tp')
- chan_gain: float32 [2048], P('tp'), may hold values from 0.1 to 1.9
- out_w: bfloat16 [2048, 2048], P('tp'), may hold values from -0.125 to 0.125
- tokens_b: bfloat16 [6144, 2048], P('ep'), may hold values from -6 to 6
- gain_b: float32 [2048], replicated, may hold values from 0.1 to 1.9
- routes: int32 [6144, 2], P('ep'), may hold values from 0 to 31, all different within a row; in each aligned block of 192 rows (0 to 191, 192 to 383, ...) at most 18 rows name the same one
- route_logits: float32 [6144, 2], P('ep'), may hold values from -6 to 6
- expert_gate: bfloat16 [32, 2048, 2816], P('ep', None, 'tp'), may hold values from -0.125 to 0.125
- expert_up: bfloat16 [32, 2048, 2816], P('ep', None, 'tp'), may hold values from -0.125 to 0.125
- expert_down: bfloat16 [32, 2816, 2048], P('ep', 'tp'), may hold values from -0.109375 to 0.109375
Outputs:
- conv_out: bfloat16 [2048, 4096], P('tp', 'ep')
- moe_out: bfloat16 [2048, 6144], P('tp', 'ep')
The draws below stay inside these ranges and needn't reach their ends.
Inputs may be any that keep to these rules, and one draw needn't show every extreme that they name: `routes`: each row names 2 different experts; among the rows of one index of ep no expert is named by more than 18 rows, a bound that some block reaches.
All inputs are finite; a program needn't handle non-finite values.
Results may differ from the reference program's by a relative error of at most 0.018.
Values may be sent and summed in bfloat16 or wider, within the bound.
A program may use at most 64 MiB of HBM per device.

```python
import math
import jax
import jax.numpy as jnp
import numpy as np
from jax import lax

D = 2048
CONV_CH = 2048
KWIDTH = 31
FF = 2816
TOPK = 2
ROWS_B = 192
EXPERTS = 32
CAP = 18
TOKENS_A = 4096
TOKENS_B = 6144
N_EP = 32
N_TP = 16


def draw_kernel(key, part):
    first, second = jax.random.split(key)
    ramp = 1.0 + 3.0 * jnp.arange(CONV_CH, dtype=jnp.float32) / CONV_CH
    base = jax.random.normal(first, (KWIDTH, CONV_CH), jnp.float32)
    rough = jax.random.uniform(second, (1, CONV_CH), jnp.float32, 0.5, 1.5)
    return base * rough * ramp[None, :] / math.sqrt(KWIDTH)


def block_scale(rng, dims, pieces, smallest, high):
    def one(position, parts):
        heights = jax.random.uniform(jax.random.fold_in(jax.random.fold_in(rng, 6), position), (parts,), jnp.float32, smallest / len(pieces), high / len(pieces))
        return jnp.repeat(jnp.exp(heights), dims[position] // parts).reshape((-1,) + (1,) * (len(dims) - position - 1))

    loudness = one(*pieces[0])
    for cut in pieces[1:]:
        loudness = loudness * one(*cut)
    return loudness


def deal_out(rng, own, number, rows, amount, top, most, slope):
    order = jax.random.permutation(rng, amount)
    heavy_load, ordinary = load_shares(amount, rows * top, most, slope, True), load_shares(amount, rows * top, most, slope, False)
    places = jnp.arange(amount)

    def named(tallies, offset_by):
        used = int((tallies > 0).sum())
        fixed = max(1, used // 4)
        passed = fixed + (places - fixed + offset_by * (used - fixed)) % max(1, amount - fixed)
        return jnp.zeros((amount,), jnp.int32).at[order[jnp.where(places < fixed, places, passed)]].set(jnp.asarray(tallies, jnp.int32))

    tallies = jnp.where(number % 4 == 0, named(heavy_load, number // 4), named(ordinary, number - number // 4 - 1))
    mixed = jax.random.permutation(jax.random.fold_in(own, 3), amount)
    source_of, taker = mixed[0:amount // 2 * 2:2], mixed[1:amount // 2 * 2:2]
    room = jnp.minimum(tallies[source_of] - 1, most - tallies[taker]) // 2
    room = jnp.where((source_of == order[0]) | (taker == order[0]) | (tallies[taker] == 0), 0, jnp.maximum(room, 0))
    passed = jax.random.randint(jax.random.fold_in(own, 4), (amount // 2,), 0, 1 << 20) % (room + 1)
    tallies = tallies.at[source_of].add(-passed).at[taker].add(passed)
    members = jnp.searchsorted(jnp.cumsum(tallies), jnp.arange(rows * top), side="right").astype(jnp.int32)
    listing = members.reshape(top, rows).T
    listing = listing[jax.random.permutation(jax.random.fold_in(own, 1), rows)]
    offset_by = jax.random.randint(jax.random.fold_in(own, 2), (rows, 1), 0, top)
    return jnp.take_along_axis(listing, (jnp.arange(top)[None, :] + offset_by) % top, axis=1)


def load_shares(count, total, bound, slope, full):
    weights = [(1 << 20) // math.isqrt(grade ** slope) + 1 for grade in range(1, count + 1)]
    largest = bound if full else min(bound, max(-(-total // count), total * weights[0] // sum(weights)))
    least = 1 if total - largest >= count - 1 else 0
    counts, spare = [largest] + [least] * (count - 1), total - largest - least * (count - 1)
    while spare > 0:
        free = [i for i in range(1, count) if counts[i] < largest] or [i for i in range(1, count) if counts[i] < bound]
        pool, budget = sum([weights[i] for i in free]), spare
        for i in free:
            more = min(bound - counts[i], max(1, budget * weights[i] // pool), spare)
            counts[i] = counts[i] + more
            spare = spare - more
    return np.array(counts)


def gaussian(own_key, dims, scale, limit, cuts=(), held_as=jnp.bfloat16):
    array = scale * jax.random.normal(own_key, dims, jnp.float32)
    if cuts:
        array = array * block_scale(own_key, dims, cuts, -0.22, 0.18)
    return jnp.clip(array, -limit, limit).astype(held_as)


def setup_inputs(seed: int = 0) -> dict:
    arg_keys = jax.random.split(jax.random.key(seed), 15)
    tokens_a = gaussian(arg_keys[0], (TOKENS_A, D), 1.0, 6.0, ((0, 32),))
    gain_a = jnp.clip(1.0 + 0.18 * jax.random.normal(arg_keys[1], (D,), jnp.float32), 0.1, 1.9)
    value_w = gaussian(arg_keys[2], (D, CONV_CH), D ** -0.5, 0.125, ((1, 16),))
    gate_w = gaussian(arg_keys[3], (D, CONV_CH), D ** -0.5, 0.125, ((1, 16),))
    kernel = draw_kernel(jax.random.fold_in(arg_keys[14], 71), 0)
    chan_gain = jnp.clip(1.0 + 0.18 * jax.random.normal(arg_keys[5], (CONV_CH,), jnp.float32), 0.1, 1.9)
    out_w = gaussian(arg_keys[6], (CONV_CH, D), CONV_CH ** -0.5, 0.125, ((0, 16),))
    tokens_b = gaussian(arg_keys[7], (TOKENS_B, D), 1.0, 6.0, ((0, 32),))
    gain_b = jnp.clip(1.0 + 0.18 * jax.random.normal(arg_keys[8], (D,), jnp.float32), 0.1, 1.9)
    routes_keys = jax.random.split(jax.random.fold_in(arg_keys[9], 1), TOKENS_B // ROWS_B)
    routes_turns = jax.random.permutation(jax.random.fold_in(arg_keys[9], 3), TOKENS_B // ROWS_B)
    routes = jax.vmap(lambda own, number: deal_out(jax.random.fold_in(arg_keys[9], 2), own, number, ROWS_B, EXPERTS, TOPK, CAP, 1))(routes_keys, routes_turns).reshape((TOKENS_B, TOPK))
    route_logits = gaussian(arg_keys[10], (TOKENS_B, TOPK), 1.0, 6.0, ((0, 32),), jnp.float32)
    expert_gate = gaussian(arg_keys[11], (EXPERTS, D, FF), D ** -0.5, 0.125, ((0, 32), (2, 16)))
    expert_up = gaussian(arg_keys[12], (EXPERTS, D, FF), D ** -0.5, 0.125, ((0, 32), (2, 16)))
    expert_down = gaussian(arg_keys[13], (EXPERTS, FF, D), FF ** -0.5, 0.109375, ((0, 32), (1, 16)))
    return dict(tokens_a=tokens_a, gain_a=gain_a, value_w=value_w, gate_w=gate_w, kernel=kernel, chan_gain=chan_gain, out_w=out_w, tokens_b=tokens_b, gain_b=gain_b, routes=routes, route_logits=route_logits, expert_gate=expert_gate, expert_up=expert_up, expert_down=expert_down)


def rms_scaled(tokens, gain):
    values = tokens.astype(jnp.float32)
    scaled = values * lax.rsqrt(lax.optimization_barrier(jnp.mean(values * values, axis=1, keepdims=True)) + 1e-06)
    return (scaled * gain[None, :]).astype(jnp.bfloat16)

def slot_table(route_rows, experts, capacity):
    flat_expert = route_rows.reshape(-1).astype(jnp.int32)
    expert_ids = jnp.arange(experts, dtype=jnp.int32)
    onehot = (flat_expert[:, None] == expert_ids[None, :]).astype(jnp.int32)
    before = jnp.cumsum(onehot, axis=0).astype(jnp.int32) - onehot
    ranking = lax.optimization_barrier(jnp.sum(before * onehot, axis=1)).astype(jnp.int32)
    return (flat_expert * capacity + ranking).astype(jnp.int32)

def reference(tokens_a, gain_a, value_w, gate_w, kernel, chan_gain, out_w, tokens_b, gain_b, routes, route_logits, expert_gate, expert_up, expert_down):
    normed = rms_scaled(tokens_a, gain_a)
    value_part = jnp.dot(normed, value_w, preferred_element_type=jnp.float32)
    gate_part = jnp.dot(normed, gate_w, preferred_element_type=jnp.float32)
    glu = (value_part * jax.nn.sigmoid(gate_part)).astype(jnp.bfloat16)
    glu = lax.optimization_barrier(glu).astype(jnp.float32)
    length = glu.shape[0]
    padded = jnp.concatenate([jnp.zeros((KWIDTH - 1, CONV_CH), jnp.float32), glu], axis=0)
    mixed = jnp.zeros((length, CONV_CH), jnp.float32)
    for tap in range(KWIDTH):
        mixed = mixed + kernel[tap][None, :] * padded[tap:tap + length]
    average = lax.optimization_barrier(jnp.mean(mixed, axis=1, keepdims=True))
    spread = lax.optimization_barrier(jnp.mean(mixed * mixed, axis=1, keepdims=True)) - average * average
    activated = jax.nn.silu((mixed - average) * lax.rsqrt(spread + 1e-05) * chan_gain[None, :]).astype(jnp.bfloat16)
    group = CONV_CH // N_TP
    conv_sum = jnp.zeros((length, D), jnp.float32)
    for index in range(N_TP):
        partial_term = jnp.dot(activated[:, index * group:(index + 1) * group], out_w[index * group:(index + 1) * group], preferred_element_type=jnp.float32).astype(jnp.bfloat16)
        conv_sum = conv_sum + lax.optimization_barrier(partial_term).astype(jnp.float32)
    conv_out = conv_sum.astype(jnp.bfloat16).T
    normed_b = rms_scaled(tokens_b, gain_b)
    per_block = TOKENS_B // N_EP
    route_blocks = routes.reshape(N_EP, per_block, TOPK)

    def block_slots(route_rows):
        return slot_table(route_rows, EXPERTS, CAP)
    slot_blocks = jax.vmap(block_slots)(route_blocks)
    block_ids = jnp.arange(N_EP, dtype=jnp.int32)
    owners = (jnp.arange(per_block * TOPK, dtype=jnp.int32) // TOPK)[None, :] + block_ids[:, None] * per_block

    def block_fill(slots, owner_rows):
        return jnp.zeros((EXPERTS * CAP,), jnp.int32).at[slots].set(owner_rows + 1)
    filled = jax.vmap(block_fill)(slot_blocks, owners)
    index_table = jnp.transpose(filled.reshape(N_EP, EXPERTS, CAP), (1, 0, 2)).reshape(EXPERTS, N_EP * CAP) - 1
    group_ff = FF // N_TP

    def expert_apply(operands):
        index_rows, gate_e, up_e, down_e = operands
        picked = jnp.take(normed_b, jnp.maximum(index_rows, 0), axis=0)
        picked = jnp.where((index_rows >= 0)[:, None], picked, jnp.zeros_like(picked))
        gate_act = jnp.dot(picked, gate_e, preferred_element_type=jnp.float32)
        up_act = jnp.dot(picked, up_e, preferred_element_type=jnp.float32)
        hidden = (jax.nn.silu(gate_act) * up_act).astype(jnp.bfloat16)
        hidden_groups = hidden.reshape(-1, N_TP, group_ff).astype(jnp.float32)
        down_groups = down_e.reshape(N_TP, group_ff, D).astype(jnp.float32)
        partial_terms = jnp.einsum('sgf,gfd->gsd', hidden_groups, down_groups).astype(jnp.bfloat16)
        partial_terms = lax.optimization_barrier(partial_terms)
        return lax.optimization_barrier(jnp.sum(partial_terms.astype(jnp.float32), axis=0)).astype(jnp.bfloat16)
    results = lax.map(expert_apply, (index_table, expert_gate, expert_up, expert_down))
    results_flat = results.reshape(EXPERTS * N_EP * CAP, D)
    expert_flat = route_blocks.reshape(N_EP, per_block * TOPK)
    ranking = slot_blocks - expert_flat * CAP
    flat_index = expert_flat * (N_EP * CAP) + block_ids[:, None] * CAP + ranking
    values = jnp.take(results_flat, flat_index.reshape(-1), axis=0).astype(jnp.float32).reshape(TOKENS_B, TOPK, D)
    weights = jax.nn.softmax(route_logits, axis=1)
    moe_out = lax.optimization_barrier(jnp.sum(weights[:, :, None] * values, axis=1)).astype(jnp.bfloat16).T
    return (conv_out, moe_out)
```

```python
import jax
import jax.numpy as jnp
from jax import lax
from jax.sharding import Mesh
from jax.sharding import PartitionSpec as P

CONV_CH = 2048
TP = ("tp_0", "tp_1")


def from_behind(block, axis, distance):
    devices = range(lax.axis_size(axis))
    route = [(i - distance, i) for i in devices if i - distance in devices]
    return lax.ppermute(block, axis, route)


def copy_for_each(x, axis):
    peers = lax.axis_size(axis)
    return lax.all_to_all(jnp.broadcast_to(x[None], (peers, *x.shape)), axis, 0, 0, tiled=True)


def taken_together(x, axis):
    return copy_for_each(x, axis).sum(axis=0)


def in_one(arrays, axis):
    ends = [0]
    for a in arrays:
        ends.append(ends[-1] + a.size)
    so_far = taken_together(jnp.concatenate([a.ravel() for a in arrays]), axis)
    return tuple((so_far[b:e].reshape(a.shape) for a, b, e in zip(arrays, ends, ends[1:])))


def in_blocks(x, dim, peers):
    before, after = (x.shape[:dim], x.shape[dim + 1 :])
    return jnp.moveaxis(x.reshape(*before, peers, -1, *after), dim, 0)


def sum_at_owner(x, axis, dim):
    peers = lax.axis_size(axis)
    tiles = lax.all_to_all(in_blocks(x, dim, peers), axis, 0, 0, tiled=True)
    return jnp.sum(tiles.astype(jnp.float32), axis=0)


def summed_rows(terms, axes):
    so_far = terms.astype(jnp.bfloat16)
    for axis in axes:
        so_far = lax.psum_scatter(so_far, axis, scatter_dimension=0, tiled=True)
    return so_far.astype(jnp.float32)


def rms_scaled(tokens, gain):
    values = tokens.astype(jnp.float32)
    scaled = values * lax.rsqrt(jnp.mean(values * values, axis=1, keepdims=True) + 1e-06)
    return (scaled * gain[None, :]).astype(jnp.bfloat16)


def slot_table(route_rows, experts, capacity):
    flat_expert = route_rows.reshape(-1)
    expert_ids = jnp.arange(experts, dtype=jnp.int32)
    onehot = (flat_expert[:, None] == expert_ids[None, :]).astype(jnp.int32)
    before = jnp.cumsum(onehot, axis=0) - onehot
    ranking = jnp.sum(before * onehot, axis=1)
    return flat_expert * capacity + ranking


def body(
    tokens_a,
    gain_a,
    value_w,
    gate_w,
    kernel,
    chan_gain,
    out_w,
    tokens_b,
    gain_b,
    routes,
    route_logits,
    expert_gate,
    expert_up,
    expert_down,
):
    normed = rms_scaled(tokens_a, gain_a)
    contract_first = (((0,), (1,)), ((), ()))
    value_part = lax.dot_general(
        value_w, normed, contract_first, preferred_element_type=jnp.float32
    )
    gate_part = lax.dot_general(gate_w, normed, contract_first, preferred_element_type=jnp.float32)
    glu = (value_part * jax.nn.sigmoid(gate_part)).astype(jnp.bfloat16)
    taps = kernel.shape[0]
    length = glu.shape[1]
    rim = from_behind(glu[:, length - (taps - 1) :], "ep", 1)
    padded = jnp.concatenate([rim, glu], axis=1).astype(jnp.float32)
    mixed = jnp.zeros(glu.shape, jnp.float32)
    for tap in range(taps):
        mixed = mixed + kernel[tap][:, None] * padded[:, tap : tap + length]
    chan_total, chan_square = in_one((jnp.sum(mixed, axis=0), jnp.sum(mixed * mixed, axis=0)), TP)
    average = chan_total / CONV_CH
    spread = chan_square / CONV_CH - average * average
    normal_out = (
        (mixed - average[None, :]) * lax.rsqrt(spread + 1e-05)[None, :] * chan_gain[:, None]
    )
    activated = jax.nn.silu(normal_out).astype(jnp.bfloat16)
    block_w = out_w
    conv_out = sum_at_owner(
        lax.dot_general(
            block_w, activated, (((0,), (0,)), ((), ())), preferred_element_type=jnp.float32
        ).astype(jnp.bfloat16),
        TP,
        0,
    ).astype(jnp.bfloat16)
    normed_b = rms_scaled(tokens_b, gain_b)
    experts = lax.axis_size("ep")
    token_count = tokens_b.shape[0]
    choices_per = routes.shape[1]
    capacity = 3 * token_count * choices_per // (2 * experts)
    slots = slot_table(routes, experts, capacity)
    owner = jnp.arange(slots.shape[0], dtype=jnp.int32) // choices_per
    filled = jnp.zeros((experts * capacity,), jnp.int32).at[slots].set(owner + 1)
    own = lax.axis_index(TP)
    width = normed_b.shape[1] // lax.axis_size(TP)
    part = lax.dynamic_slice_in_dim(normed_b, own * width, width, axis=1)
    picked = jnp.take(part, jnp.maximum(filled - 1, 0), axis=0)
    send_rows = jnp.where((filled > 0)[:, None], picked, jnp.zeros_like(picked)).reshape(
        experts, capacity, -1
    )
    weights = jax.nn.softmax(route_logits, axis=1).reshape(-1)
    slot_ids = jnp.arange(experts * capacity, dtype=jnp.int32)
    combine = (
        ((slots[:, None] == slot_ids[None, :]).astype(jnp.float32) * weights[:, None])
        .reshape(token_count, choices_per, -1)
        .sum(axis=1)
    )
    gate_local = expert_gate[0]
    up_local = expert_up[0]
    arrived = lax.all_to_all(send_rows, "ep", split_axis=0, concat_axis=0, tiled=True).reshape(
        experts * capacity, -1
    )
    arrived = lax.all_gather(arrived, TP, axis=1, tiled=True)
    gate_act = jnp.dot(arrived, gate_local, preferred_element_type=jnp.float32)
    up_act = jnp.dot(arrived, up_local, preferred_element_type=jnp.float32)
    hidden = (jax.nn.silu(gate_act) * up_act).astype(jnp.bfloat16)
    down_local = expert_down[0]
    block_w = down_local
    expert_rows = summed_rows(
        lax.dot_general(
            block_w, hidden, (((0,), (1,)), ((), ())), preferred_element_type=jnp.float32
        ),
        TP,
    ).astype(jnp.bfloat16)
    returned = lax.all_to_all(
        expert_rows.reshape(expert_rows.shape[0], experts, capacity),
        "ep",
        split_axis=1,
        concat_axis=1,
        tiled=True,
    )
    returned_flat = returned.reshape(returned.shape[0], -1).astype(jnp.float32)
    moe_out = lax.dot_general(
        returned_flat,
        combine,
        (((1,), (1,)), ((), ())),
        precision=lax.Precision.HIGHEST,
        preferred_element_type=jnp.float32,
    )
    return (conv_out, moe_out.astype(jnp.bfloat16))


def solution(mesh):
    finer = Mesh(mesh.devices.reshape(mesh.shape["ep"], 8, 2), ("ep", "tp_0", "tp_1"))
    return jax.shard_map(
        body,
        mesh=finer,
        in_specs=(
            P("ep", None),
            P(),
            P(None, TP),
            P(None, TP),
            P(None, TP),
            P(TP),
            P(TP, None),
            P("ep", None),
            P(),
            P("ep", None),
            P("ep", None),
            P("ep", None, TP),
            P("ep", None, TP),
            P("ep", TP, None),
        ),
        out_specs=(P(TP, "ep"), P(TP, "ep")),
        check_vma=False,
    )
```

```python
import functools
from types import SimpleNamespace

import jax
import jax.numpy as jnp
from jax import lax
from jax.experimental import pallas as pl
from jax.experimental.pallas import tpu as pltpu
from jax.sharding import PartitionSpec as P

MESH = pl.DeviceIdType.MESH
BF = jnp.bfloat16
F32 = jnp.float32
I32 = jnp.int32
MAIN = 16
INPUTS = (
    "tok_b", "routes", "logits", "gain_b", "tok_a", "gain_a", "vw", "gw",
    "ker", "cg", "ow", "eg", "eu", "ed",
)


def iota(shape, dim):
    return lax.broadcasted_iota(I32, shape, dim)


def dot(a, b, ca=1, cb=0, precision=None):
    return lax.dot_general(
        a, b, (((ca,), (cb,)), ((), ())), precision=precision, preferred_element_type=F32
    )


def silu(v):
    return v / (1.0 + jnp.exp(-v))


def kernel(g, *refs):
    r = SimpleNamespace(**dict(zip(g.names, refs)))
    Z, X, Y, F, EX, EXT = g.Z, g.X, g.Y, g.F, g.EX, g.EXT
    NT, T, R, D, S = g.NT, g.T, g.R, g.D, g.S
    M = EX * MAIN
    HALF = M // 2
    H = Y // 2
    e = lax.axis_index("ep")
    t = lax.axis_index("tp")
    core, y = lax.rem(t, 2), lax.div(t, 2)
    z, x = lax.div(e, X), lax.rem(e, X)
    way = 1 - 2 * core
    mate = (e, t + way)
    mine = pl.ds(pl.multiple_of(core * F, F), F)

    def turn(a):
        return lax.rem(a + 4 * Y, Y)

    def tp_of(step):
        return (e, turn(y + step) * 2 + core)

    def place(b):
        i, dx = b // X, b % X
        dz = jnp.where(i % 2 == 1, (i + 1) // 2, Z - i // 2)
        return lax.rem(z + dz, Z) * X + lax.rem(x + dx, X)

    def opposite(b):
        i, dx = b // X, b % X
        back = jnp.where((i == 0) | (i == Z - 1), i, jnp.where(i % 2 == 1, i + 1, i - 1))
        return back * X + lax.rem(X - dx, X)

    def remote(src, dst, send, recv, to):
        return pltpu.make_async_remote_copy(
            src_ref=src, dst_ref=dst, send_sem=send, recv_sem=recv, device_id=to, device_id_type=MESH
        )

    barrier = pltpu.get_barrier_semaphore()

    def greet_ep(i, c):
        pl.semaphore_signal(barrier, 1, device_id=(lax.rem(e + i, EX), t), device_id_type=MESH)
        return c

    def greet_tp(i, c):
        pl.semaphore_signal(barrier, 1, device_id=(e, lax.rem(t + i, NT)), device_id_type=MESH)
        return c

    lax.fori_loop(1, EX, greet_ep, 0)
    lax.fori_loop(1, NT, greet_tp, 0)

    loads = {}
    for i, name in enumerate(INPUTS):
        loads[name] = pltpu.make_async_copy(
            getattr(r, "in_" + name), getattr(r, "v_" + name), r.in_sem.at[i]
        )
        loads[name].start()

    for name in ("tok_b", "gain_b", "routes", "logits"):
        loads[name].wait()
    squares = jnp.zeros((R, F), F32)
    for j in range(NT):
        v = r.v_tok_b[:, j * F : (j + 1) * F].astype(F32)
        squares = squares + v * v
    inv = lax.rsqrt(jnp.sum(squares, axis=1, keepdims=True) / D + 1e-6)
    own = r.v_tok_b[:, pl.ds(pl.multiple_of(t * F, F), F)].astype(F32)
    normed = (own * inv * r.v_gain_b[pl.ds(t, 1), :]).astype(BF)

    lines = iota((EX, R), 0)
    first = jnp.where(lines == r.v_routes[0:1, :], 1.0, 0.0)
    second = jnp.where(lines == r.v_routes[1:2, :], 1.0, 0.0)
    named = first + second
    earlier = jnp.where(iota((R, R), 0) < iota((R, R), 1), 1.0, 0.0).astype(BF)
    code = (named * (dot(named.astype(BF), earlier) + 1.0)).astype(BF)
    l0, l1 = r.v_logits[0:1, :], r.v_logits[1:2, :]
    top = jnp.maximum(l0, l1)
    e0, e1 = jnp.exp(l0 - top), jnp.exp(l1 - top)
    weight = first * (e0 / (e0 + e1)) + second * (e1 / (e0 + e1))
    w_hi = weight.astype(BF)
    w_lo = (weight - w_hi.astype(F32)).astype(BF)

    s = iota((S, EX), 0)
    block = jnp.where(s < M, s // MAIN, (s - M) // EXT)
    spread = jnp.where(iota((S, EX), 1) == place(block), 1.0, 0.0).astype(BF)
    q = iota((S, R), 0)
    rank = jnp.where(q < M, q % MAIN, MAIN + (q - M) % EXT) + 1
    pick = dot(spread, code) == rank.astype(F32)
    r.w_hi[...] = jnp.where(pick, dot(spread, w_hi), 0.0).astype(BF)
    r.w_lo[...] = jnp.where(pick, dot(spread, w_lo), 0.0).astype(BF)
    rows = dot(jnp.where(pick, 1.0, 0.0).astype(BF), normed)
    r.send_main[...] = rows[:M].astype(BF)
    r.ag[0, 0:MAIN, mine] = rows[:MAIN].astype(BF)
    r.rows_ext[...] = rows[M:]
    for b in range(EX):
        r.send_ext[b] = r.rows_ext[b * EXT : (b + 1) * EXT, :].astype(BF)
    r.recv_ext[0] = r.rows_ext[0:EXT, :].astype(BF)

    pl.semaphore_wait(barrier, EX - 1 + NT - 1)

    def dispatch(b, c):
        to, nb = (place(b), t), opposite(b)
        remote(
            r.send_main.at[pl.ds(pl.multiple_of(b * MAIN, MAIN), MAIN), :],
            r.ag.at[0, pl.ds(pl.multiple_of(nb * MAIN, MAIN), MAIN), mine],
            r.out_sem.at[0], r.a2a_sem.at[nb // (EX // 2)], to,
        ).start()
        remote(
            r.send_ext.at[b], r.recv_ext.at[nb], r.out_sem.at[1], r.a2a_sem.at[2], to
        ).start()
        return c

    lax.fori_loop(1, EX, dispatch, 0)

    for name in ("tok_a", "gain_a", "vw", "gw"):
        loads[name].wait()
    squares = jnp.zeros((T, F), F32)
    for j in range(NT):
        v = r.v_tok_a[:, j * F : (j + 1) * F].astype(F32)
        squares = squares + v * v
    inv = lax.rsqrt(jnp.sum(squares, axis=1, keepdims=True) / D + 1e-6)
    for j in range(NT):
        cols = slice(j * F, (j + 1) * F)
        v = r.v_tok_a[:, cols].astype(F32) * inv * r.v_gain_a[j : j + 1, :]
        r.normed_a[:, cols] = v.astype(BF)
    value = dot(r.normed_a[...], r.v_vw[...])
    gate = dot(r.normed_a[...], r.v_gw[...])
    glu = (value / (1.0 + jnp.exp(-gate))).astype(BF)
    r.padded[32:, :] = glu.astype(F32)
    r.tail[...] = glu[T - 32 :, :]
    halo = remote(r.tail, r.halo, r.out_sem.at[2], r.halo_sem, (lax.rem(e + 1, EX), t))
    halo.start()

    loads["ker"].wait()
    halo.wait_recv()
    r.padded[0:32, :] = jnp.where(e > 0, r.halo[...].astype(F32), 0.0)
    mixed = jnp.zeros((T, F), F32)
    for tap in range(g.TAPS):
        low = 32 - (g.TAPS - 1) + tap
        mixed = mixed + r.v_ker[tap : tap + 1, :] * r.padded[low : low + T, :]
    r.mixed[...] = mixed
    ones = jnp.ones((8, F), F32)
    sums = dot(ones, mixed, 1, 1, lax.Precision.HIGHEST)
    powers = dot(ones, mixed * mixed, 1, 1, lax.Precision.HIGHEST)
    r.stats[0] = jnp.where(iota((8, T), 0) == 0, sums, powers)[0:2]

    def tell(i, c):
        remote(
            r.stats.at[0], r.stats.at[NT - i], r.out_sem.at[3], r.stat_sem, (e, lax.rem(t + i, NT))
        ).start()
        return c

    lax.fori_loop(1, NT, tell, 0)

    pieces = (pl.ds(0, HALF), pl.ds(HALF, S - HALF))

    def pass_on(slot, to_slot, piece, step):
        return remote(
            r.ag.at[slot, pieces[piece], mine], r.ag.at[to_slot, pieces[piece], mine],
            r.ag_out.at[to_slot, piece], r.ag_in.at[to_slot, piece], tp_of(step),
        )

    def to_mate(slot):
        return remote(
            r.ag.at[slot, :, mine], r.ag.at[slot, :, mine], r.am_out.at[slot], r.am_in.at[slot], mate
        )

    def bulk(ref, sem):
        return pltpu.make_async_copy(ref, ref, sem)

    for piece in (0, 1):
        if piece == 0:
            bulk(r.ag.at[0, pl.ds(MAIN, HALF - MAIN), mine], r.a2a_sem.at[0]).wait()
        else:
            bulk(r.ag.at[0, pl.ds(HALF, HALF), mine], r.a2a_sem.at[1]).wait()
            bulk(r.recv_ext.at[pl.ds(1, EX - 1)], r.a2a_sem.at[2]).wait()
            for b in range(EX):
                r.rows_ext[b * EXT : (b + 1) * EXT, :] = r.recv_ext[b].astype(F32)
            r.ag[0, M:S, mine] = r.rows_ext[...].astype(BF)
        pass_on(0, turn(-way), piece, way).start()
        pass_on(0, turn(way), piece, -way).start()
    to_mate(0).start()

    loads["cg"].wait()
    loads["ow"].wait()
    bulk(r.stats.at[pl.ds(1, NT - 1)], r.stat_sem).wait()
    total = r.stats[0]
    for j in range(1, NT):
        total = total + r.stats[j]
    average = total[0:1] / g.CH
    scale = lax.rsqrt(total[1:2] / g.CH - average * average + 1e-5)
    line = iota((8, T), 0)
    both = jnp.where(line == 0, average, jnp.where(line == 1, scale, 0.0))
    line = iota((8, F), 0)
    high = lax.Precision.HIGHEST
    average = dot(both, jnp.where(line == 0, 1.0, 0.0), 0, 0, high)
    scale = dot(both, jnp.where(line == 1, 1.0, 0.0), 0, 0, high)
    act = silu((r.mixed[...] - average) * scale * r.v_cg[...]).astype(BF)
    for j in range(NT):
        r.c_part[j] = dot(act, r.v_ow[:, j * F : (j + 1) * F]).astype(BF)

    def c_mate(slot):
        return remote(
            r.c_part.at[turn(y + slot) * 2 + 1 - core], r.c_pair.at[slot],
            r.cm_out.at[slot], r.cm_in.at[slot], mate,
        )

    for slot in range(Y):
        c_mate(slot).start()

    def c_sum(slot):
        c_mate(slot).wait_recv()
        mine_part = r.c_part[turn(y + slot) * 2 + core].astype(F32)
        return mine_part + r.c_pair[slot].astype(F32)

    def c_link(slot, to_slot, step):
        return remote(
            r.c_stage.at[slot], r.c_got.at[to_slot], r.c_out.at[to_slot], r.c_in.at[to_slot], tp_of(step)
        )

    def c_step(k, sign):
        slot = turn(sign * k * way)
        last = 0 if sign > 0 else Y
        to_slot = last if k == 1 else turn(sign * (k - 1) * way)
        part = c_sum(slot)
        if k < (H if sign > 0 else H - 1):
            c_link(slot, slot, 0).wait_recv()
            part = part + r.c_got[slot].astype(F32)
        r.c_stage[slot] = part.astype(BF)
        c_link(slot, to_slot, sign * way).start()

    loads["eg"].wait()
    loads["eu"].wait()
    TILE = S // g.TILES

    def experts_in(slot, first):
        cols = pl.ds(pl.multiple_of(turn(y + slot) * 2 * F, 2 * F), 2 * F)
        wg, wu = r.v_eg[:, cols], r.v_eu[:, cols]
        for i in range(g.TILES):
            part = pl.ds(i * TILE, TILE)
            lhs = r.ag[slot, part, :]
            a, b = dot(lhs, wg, 1, 1), dot(lhs, wu, 1, 1)
            r.gate[part, :] = a if first else r.gate[part, :] + a
            r.up[part, :] = b if first else r.up[part, :] + b

    waiting = [0]
    for k in range(1, H + 1):
        for piece in (0, 1):
            down, up = turn(-k * way), turn(k * way)
            pass_on(0, down, piece, way).wait_recv()
            if k < H:
                pass_on(down, turn(-(k + 1) * way), piece, way).start()
                pass_on(0, up, piece, -way).wait_recv()
                if k < H - 1:
                    pass_on(up, turn((k + 1) * way), piece, -way).start()
        to_mate(down).start()
        if k < H:
            to_mate(up).start()
        c_step(H - k + 1, 1)
        if k > 1:
            c_step(H - k + 1, -1)
        for slot in waiting:
            to_mate(slot).wait_recv()
            experts_in(slot, k == 1)
        waiting = [down, up] if k < H else [down]
    for slot in waiting:
        to_mate(slot).wait_recv()
        experts_in(slot, False)
    r.hidden[...] = (silu(r.gate[...]) * r.up[...]).astype(BF)
    loads["ed"].wait()

    def down_cols(slot, who):
        return pl.ds(pl.multiple_of((turn(y + slot) * 2 + who) * F, F), F)

    def m_mate(slot):
        return remote(r.m_part.at[slot], r.m_pair.at[slot], r.mm_out.at[slot], r.mm_in.at[slot], mate)

    order = [turn(H * way)]
    for k in range(H - 1, 0, -1):
        order += [turn(k * way), turn(-k * way)]
    order += [0]
    for slot in order:
        r.m_part[slot] = dot(r.hidden[...], r.v_ed[:, down_cols(slot, 1 - core)]).astype(BF)
        m_mate(slot).start()

    def m_link(slot, to_slot, piece, step):
        return remote(
            r.m_stage.at[slot, pieces[piece], :], r.m_got.at[to_slot, pieces[piece], :],
            r.m_out.at[to_slot, piece], r.m_in.at[to_slot, piece], tp_of(step),
        )

    def m_step(k, sign, piece):
        slot = turn(sign * k * way)
        last = 0 if sign > 0 else Y
        to_slot = last if k == 1 else turn(sign * (k - 1) * way)
        part = pieces[piece]
        if piece == 0:
            m_mate(slot).wait_recv()
        total = dot(r.hidden[part, :], r.v_ed[:, down_cols(slot, core)])
        total = total + r.m_pair[slot, part, :].astype(F32)
        if k < (H if sign > 0 else H - 1):
            m_link(slot, slot, piece, 0).wait_recv()
            total = total + r.m_got[slot, part, :].astype(F32)
        r.m_stage[slot, part, :] = total.astype(BF)
        m_link(slot, to_slot, piece, sign * way).start()

    for k in range(H, 0, -1):
        for piece in (0, 1):
            m_step(k, 1, piece)
            if k < H:
                m_step(k, -1, piece)

    for piece in (0, 1):
        part = pieces[piece]
        if piece == 0:
            m_mate(0).wait_recv()
        total = dot(r.hidden[part, :], r.v_ed[:, down_cols(0, core)])
        total = total + r.m_pair[0, part, :].astype(F32)
        m_link(0, 0, piece, 0).wait_recv()
        total = total + r.m_got[0, part, :].astype(F32)
        m_link(0, Y, piece, 0).wait_recv()
        total = total + r.m_got[Y, part, :].astype(F32)
        r.back[part, :] = total.astype(BF)
        if piece == 1:
            r.rows_ext[...] = total[M - HALF :]
            for b in range(EX):
                r.back_ext[b] = r.rows_ext[b * EXT : (b + 1) * EXT, :].astype(BF)

        def give_back(b, c):
            to, nb = (place(b), t), opposite(b)
            remote(
                r.back.at[pl.ds(pl.multiple_of(b * MAIN, MAIN), MAIN), :],
                r.home.at[pl.ds(pl.multiple_of(nb * MAIN, MAIN), MAIN), :],
                r.out_sem.at[4], r.home_sem.at[0], to,
            ).start()
            return c

        def give_ext(b, c):
            remote(
                r.back_ext.at[b], r.home_ext.at[opposite(b)], r.out_sem.at[5], r.home_sem.at[1],
                (place(b), t),
            ).start()
            return c

        if piece == 0:
            lax.fori_loop(1, EX // 2, give_back, 0)
        else:
            lax.fori_loop(EX // 2, EX, give_back, 0)
            lax.fori_loop(1, EX, give_ext, 0)
    r.home[0:MAIN, :] = r.back[0:MAIN, :]
    r.home_ext[0] = r.back_ext[0]

    total = c_sum(0)
    c_link(0, 0, 0).wait_recv()
    total = total + r.c_got[0].astype(F32)
    c_link(0, Y, 0).wait_recv()
    total = total + r.c_got[Y].astype(F32)
    r.conv_out[...] = jnp.transpose(total).astype(BF)

    bulk(r.home.at[pl.ds(MAIN, M - MAIN), :], r.home_sem.at[0]).wait()
    bulk(r.home_ext.at[pl.ds(1, EX - 1)], r.home_sem.at[1]).wait()
    for b in range(EX):
        r.rows_ext[b * EXT : (b + 1) * EXT, :] = r.home_ext[b].astype(F32)
    r.home[M:S, :] = r.rows_ext[...].astype(BF)
    result = dot(r.home[...], r.w_hi[...], 0, 0) + dot(r.home[...], r.w_lo[...], 0, 0)
    r.moe_out[...] = result.astype(BF)

    bulk(r.send_main.at[pl.ds(MAIN, M - MAIN), :], r.out_sem.at[0]).wait()
    bulk(r.send_ext.at[pl.ds(1, EX - 1)], r.out_sem.at[1]).wait()
    halo.wait_send()
    bulk(r.stats.at[pl.ds(1, NT - 1)], r.out_sem.at[3]).wait()
    bulk(r.back.at[pl.ds(MAIN, M - MAIN), :], r.out_sem.at[4]).wait()
    bulk(r.back_ext.at[pl.ds(1, EX - 1)], r.out_sem.at[5]).wait()
    for slot in range(Y):
        to_mate(slot).wait_send()
        c_mate(slot).wait_send()
        m_mate(slot).wait_send()
    for slot in range(1, Y):
        for piece in (0, 1):
            pass_on(0, slot, piece, 0).wait_send()
    final = [0, Y] + [turn(k * way) for k in range(1, H)] + [turn(-k * way) for k in range(1, H - 1)]
    for slot in final:
        c_link(0, slot, 0).wait_send()
        for piece in (0, 1):
            m_link(0, slot, piece, 0).wait_send()


def run(Z, X, args):
    (tok_a, gain_a, vw, gw, ker, cg, ow, tok_b, gain_b, routes, logits, eg, eu, ed) = args
    EX, NT = lax.axis_size("ep"), lax.axis_size("tp")
    T, D = tok_a.shape
    R, F, HU = tok_b.shape[0], vw.shape[1], eg.shape[2]
    cap = 3 * R * routes.shape[1] // (2 * EX)
    EXT, Y = cap - MAIN, NT // 2
    S, M = EX * cap, EX * MAIN
    given = dict(
        tok_b=tok_b, routes=routes.T, logits=logits.T, gain_b=gain_b.reshape(NT, F),
        tok_a=tok_a, gain_a=gain_a.reshape(NT, F), vw=vw, gw=gw, ker=ker, cg=cg.reshape(1, F),
        ow=ow, eg=eg[0].T, eu=eu[0].T, ed=ed[0],
    )
    vm, dma = pltpu.VMEM, pltpu.SemaphoreType.DMA
    scratch = dict(
        {"v_" + n: vm(given[n].shape, given[n].dtype) for n in INPUTS},
        in_sem=dma((len(INPUTS),)), w_hi=vm((S, R), BF), w_lo=vm((S, R), BF),
        send_main=vm((M, F), BF), send_ext=vm((EX, EXT, F), BF), recv_ext=vm((EX, EXT, F), BF),
        rows_ext=vm((EX * EXT, F), F32), ag=vm((Y, S, 2 * F), BF),
        out_sem=dma((6,)), a2a_sem=dma((3,)), normed_a=vm((T, D), BF), padded=vm((T + 32, F), F32),
        tail=vm((32, F), BF), halo=vm((32, F), BF), halo_sem=dma, mixed=vm((T, F), F32),
        stats=vm((NT, 2, T), F32), stat_sem=dma,
        ag_out=dma((Y, 2)), ag_in=dma((Y, 2)), am_out=dma((Y,)), am_in=dma((Y,)),
        c_part=vm((NT, T, F), BF), c_pair=vm((Y, T, F), BF), c_stage=vm((Y, T, F), BF),
        c_got=vm((Y + 1, T, F), BF), cm_out=dma((Y,)), cm_in=dma((Y,)), c_out=dma((Y + 1,)),
        c_in=dma((Y + 1,)), gate=vm((S, HU), F32), up=vm((S, HU), F32), hidden=vm((S, HU), BF),
        m_part=vm((Y, S, F), BF), m_pair=vm((Y, S, F), BF), m_stage=vm((Y, S, F), BF),
        m_got=vm((Y + 1, S, F), BF), mm_out=dma((Y,)), mm_in=dma((Y,)), m_out=dma((Y + 1, 2)),
        m_in=dma((Y + 1, 2)), back=vm((S, F), BF), back_ext=vm((EX, EXT, F), BF),
        home=vm((S, F), BF), home_ext=vm((EX, EXT, F), BF), home_sem=dma((2,)),
    )
    names = ["in_" + n for n in INPUTS] + ["conv_out", "moe_out"] + list(scratch)
    g = SimpleNamespace(
        names=names, Z=Z, X=X, Y=Y, F=F, EX=EX, EXT=EXT, NT=NT, T=T, R=R, D=D, S=S, CH=NT * F,
        TAPS=ker.shape[0], TILES=3,
    )
    return pl.pallas_call(
        functools.partial(kernel, g),
        out_shape=(jax.ShapeDtypeStruct((F, T), BF), jax.ShapeDtypeStruct((F, R), BF)),
        in_specs=[pl.BlockSpec(memory_space=pl.ANY)] * len(INPUTS),
        out_specs=(pl.BlockSpec(memory_space=pltpu.VMEM),) * 2,
        scratch_shapes=list(scratch.values()),
        compiler_params=pltpu.CompilerParams(
            collective_id=0, has_side_effects=True, vmem_limit_bytes=60 * 1024 * 1024
        ),
    )(*[given[n] for n in INPUTS])


def solution(mesh, Z=8, X=4):
    return jax.shard_map(
        lambda *args: run(Z, X, args),
        mesh=mesh,
        in_specs=(
            P("ep", None), P(), P(None, "tp"), P(None, "tp"), P(None, "tp"), P("tp"), P("tp", None),
            P("ep", None), P(), P("ep", None), P("ep", None), P("ep", None, "tp"),
            P("ep", None, "tp"), P("ep", "tp", None),
        ),
        out_specs=(P("tp", "ep"), P("tp", "ep")),
        check_vma=False,
    )
```

```python
import functools
from types import SimpleNamespace

import jax
import jax.numpy as jnp
from jax import lax
from jax.experimental import pallas as pl
from jax.experimental.pallas import tpu as pltpu
from jax.sharding import PartitionSpec as P

MESH = pl.DeviceIdType.MESH
BF = jnp.bfloat16
F32 = jnp.float32
I32 = jnp.int32
MAIN = 16
INPUTS = (
    "tok_b", "routes", "logits", "gain_b", "tok_a", "gain_a", "vw", "gw",
    "ker", "cg", "ow", "eg", "eu", "ed",
)


def iota(shape, dim):
    return lax.broadcasted_iota(I32, shape, dim)


def dot(a, b, ca=1, cb=0, precision=None):
    return lax.dot_general(
        a, b, (((ca,), (cb,)), ((), ())), precision=precision, preferred_element_type=F32
    )


def silu(v):
    return v / (1.0 + jnp.exp(-v))


def kernel(g, *refs):
    r = SimpleNamespace(**dict(zip(g.names, refs)))
    Z, X, Y, F, EX, EXT = g.Z, g.X, g.Y, g.F, g.EX, g.EXT
    NT, T, R, D, S = g.NT, g.T, g.R, g.D, g.S
    M = EX * MAIN
    HALF = M // 2
    H, DN = Y // 2, g.DN
    LA, LB = H - (DN + 1) // 2, H - 1 - DN // 2
    e = lax.axis_index("ep")
    t = lax.axis_index("tp")
    core, y = lax.rem(t, 2), lax.div(t, 2)
    z, x = lax.div(e, X), lax.rem(e, X)
    way = 1 - 2 * core
    mate = (e, t + way)
    mine = pl.ds(pl.multiple_of(core * F, F), F)
    other = pl.ds(pl.multiple_of((1 - core) * F, F), F)
    near = H - 1 + core if DN == 2 else H - DN // 2

    def turn(a):
        return lax.rem(a + 4 * Y, Y)

    def tp_of(step):
        return (e, turn(y + step) * 2 + core)

    def place(b):
        i, dx = b // X, b % X
        dz = jnp.where(i % 2 == 1, (i + 1) // 2, Z - i // 2)
        return lax.rem(z + dz, Z) * X + lax.rem(x + dx, X)

    rows_of = [lax.rem(z + i, Z) * X for i in range(Z)]
    cols_of = [lax.rem(x + i, X) for i in range(X)]

    def peer(b):
        i, dx = divmod(b, X)
        dz = ((i + 1) // 2 if i % 2 else Z - i // 2) % Z
        return (rows_of[dz] + cols_of[dx], t)

    def opposite(b):
        i, dx = divmod(b, X)
        back = i if i in (0, Z - 1) else (i + 1 if i % 2 else i - 1)
        return back * X + (X - dx) % X

    def remote(src, dst, send, recv, to):
        return pltpu.make_async_remote_copy(
            src_ref=src, dst_ref=dst, send_sem=send, recv_sem=recv, device_id=to, device_id_type=MESH
        )

    barrier = pltpu.get_barrier_semaphore()

    for b in range(EX - 1, 0, -1):
        pl.semaphore_signal(barrier, 1, device_id=peer(b), device_id_type=MESH)
    tps = [(e, lax.rem(t + i, NT)) for i in range(NT)]
    for i in range(1, NT):
        pl.semaphore_signal(barrier, 1, device_id=tps[i], device_id_type=MESH)

    loads = {}
    for i, name in enumerate(INPUTS):
        loads[name] = pltpu.make_async_copy(
            getattr(r, "in_" + name), getattr(r, "v_" + name), r.in_sem.at[i]
        )
        loads[name].start()

    for name in ("tok_b", "gain_b", "routes", "logits"):
        loads[name].wait()
    squares = jnp.zeros((R, F), F32)
    for j in range(NT):
        v = r.v_tok_b[:, j * F : (j + 1) * F].astype(F32)
        squares = squares + v * v
    inv = lax.rsqrt(jnp.sum(squares, axis=1, keepdims=True) / D + 1e-6)

    lines = iota((EX, R), 0)
    first = jnp.where(lines == r.v_routes[0:1, :], 1.0, 0.0)
    second = jnp.where(lines == r.v_routes[1:2, :], 1.0, 0.0)
    named = first + second
    earlier = jnp.where(iota((R, R), 0) < iota((R, R), 1), 1.0, 0.0).astype(BF)
    code = (named * (dot(named.astype(BF), earlier) + 1.0)).astype(BF)
    l0, l1 = r.v_logits[0:1, :], r.v_logits[1:2, :]
    top = jnp.maximum(l0, l1)
    e0, e1 = jnp.exp(l0 - top), jnp.exp(l1 - top)
    weight = first * (e0 / (e0 + e1)) + second * (e1 / (e0 + e1))
    w_hi = weight.astype(BF)
    w_lo = (weight - w_hi.astype(F32)).astype(BF)

    s = iota((S, EX), 0)
    block = jnp.where(s < M, s // MAIN, (s - M) // EXT)
    spread = jnp.where(iota((S, EX), 1) == place(block), 1.0, 0.0).astype(BF)
    q = iota((S, R), 0)
    rank = jnp.where(q < M, q % MAIN, MAIN + (q - M) % EXT) + 1
    pick = dot(spread, code) == rank.astype(F32)
    r.w_hi[...] = jnp.where(pick, dot(spread, w_hi), 0.0).astype(BF)
    r.w_lo[...] = jnp.where(pick, dot(spread, w_lo), 0.0).astype(BF)
    picks = jnp.where(pick, 1.0, 0.0).astype(BF)

    for i in range(DN + 1):
        slot = 0 if i == 0 else near + i - 1
        col = turn(y + slot) * 2 + core
        own = r.v_tok_b[:, pl.ds(pl.multiple_of(col * F, F), F)].astype(F32)
        normed = (own * inv * r.v_gain_b[pl.ds(col, 1), :]).astype(BF)
        rows = dot(picks, normed)
        r.send_main[i] = rows[:M].astype(BF)
        r.ag[slot, 0:MAIN, mine] = rows[:MAIN].astype(BF)
        r.rows_ext[...] = rows[M:]
        for b in range(EX):
            r.send_ext[i, b] = r.rows_ext[b * EXT : (b + 1) * EXT, :].astype(BF)
        r.recv_ext[i, 0] = r.rows_ext[0:EXT, :].astype(BF)

    for name in ("tok_a", "gain_a", "vw", "gw"):
        loads[name].wait()
    squares = jnp.zeros((T, F), F32)
    for j in range(NT):
        v = r.v_tok_a[:, j * F : (j + 1) * F].astype(F32)
        squares = squares + v * v
    inv = lax.rsqrt(jnp.sum(squares, axis=1, keepdims=True) / D + 1e-6)
    for j in range(NT):
        cols = slice(j * F, (j + 1) * F)
        v = r.v_tok_a[:, cols].astype(F32) * inv * r.v_gain_a[j : j + 1, :]
        r.normed_a[:, cols] = v.astype(BF)
    value = dot(r.normed_a[...], r.v_vw[...])
    gate = dot(r.normed_a[...], r.v_gw[...])
    glu = (value / (1.0 + jnp.exp(-gate))).astype(BF)
    r.padded[32:, :] = glu.astype(F32)
    r.tail[...] = glu[T - 32 :, :]
    halo = remote(r.tail, r.halo, r.out_sem.at[4], r.halo_sem, (lax.rem(e + 1, EX), t))

    pl.semaphore_wait(barrier, EX - 1 + NT - 1)

    for b in range(1, EX):
        nb = opposite(b)
        remote(
            r.send_main.at[0, pl.ds(b * MAIN, MAIN), :], r.ag.at[0, pl.ds(nb * MAIN, MAIN), mine],
            r.out_sem.at[0], r.a2a_sem.at[nb // (EX // 2)], peer(b),
        ).start()
        remote(
            r.send_ext.at[0, b], r.recv_ext.at[0, nb], r.out_sem.at[1], r.a2a_sem.at[2], peer(b)
        ).start()
    halo.start()
    for b in range(1, EX if DN else 0):
        nb = opposite(b)
        remote(
            r.send_main.at[pl.ds(1, DN), pl.ds(b * MAIN, MAIN), :],
            r.ag.at[pl.ds(near, DN), pl.ds(nb * MAIN, MAIN), mine],
            r.out_sem.at[2], r.a2a_sem.at[3], peer(b),
        ).start()
        remote(
            r.send_ext.at[pl.ds(1, DN), b], r.recv_ext.at[pl.ds(1, DN), nb],
            r.out_sem.at[3], r.a2a_sem.at[4], peer(b),
        ).start()

    cuts = [(EX * i // 4) * MAIN for i in range(4)] + [S]
    pieces = [pl.ds(a, b - a) for a, b in zip(cuts, cuts[1:])]

    def pass_on(slot, to_slot, piece, step):
        return remote(
            r.ag.at[slot, pieces[piece], mine], r.ag.at[to_slot, pieces[piece], mine],
            r.ag_out.at[to_slot, piece], r.ag_in.at[to_slot, piece], tp_of(step),
        )

    def to_mate(slot):
        return remote(
            r.ag.at[slot, :, mine], r.ag.at[slot, :, mine], r.am_out.at[slot], r.am_in.at[slot], mate
        )

    def bulk(ref, sem):
        return pltpu.make_async_copy(ref, ref, sem)

    def settle_ext(i, slot):
        for b in range(EX):
            r.rows_ext[b * EXT : (b + 1) * EXT, :] = r.recv_ext[i, b].astype(F32)
        r.ag[slot, M:S, mine] = r.rows_ext[...].astype(BF)

    bulk(r.ag.at[0, pl.ds(MAIN, HALF - MAIN), mine], r.a2a_sem.at[0]).wait()
    for piece in (0, 1):
        pass_on(0, turn(-way), piece, way).start()
        if LB:
            pass_on(0, turn(way), piece, -way).start()
    bulk(r.ag.at[0, pl.ds(HALF, HALF), mine], r.a2a_sem.at[1]).wait()
    bulk(r.recv_ext.at[0, pl.ds(1, EX - 1)], r.a2a_sem.at[2]).wait()
    settle_ext(0, 0)
    for piece in (2, 3):
        pass_on(0, turn(-way), piece, way).start()
        if LB:
            pass_on(0, turn(way), piece, -way).start()
    to_mate(0).start()

    def convolve():
        loads["ker"].wait()
        halo.wait_recv()
        r.padded[0:32, :] = jnp.where(e > 0, r.halo[...].astype(F32), 0.0)
        mixed = jnp.zeros((T, F), F32)
        for tap in range(g.TAPS):
            low = 32 - (g.TAPS - 1) + tap
            mixed = mixed + r.v_ker[tap : tap + 1, :] * r.padded[low : low + T, :]
        r.mixed[...] = mixed
        ones = jnp.ones((8, F), F32)
        sums = dot(ones, mixed, 1, 1, lax.Precision.HIGHEST)
        powers = dot(ones, mixed * mixed, 1, 1, lax.Precision.HIGHEST)
        r.stats[0] = jnp.where(iota((8, T), 0) == 0, sums, powers)[0:2]

        for i in range(1, NT):
            remote(
                r.stats.at[0], r.stats.at[NT - i], r.out_sem.at[5], r.stat_sem, tps[i]
            ).start()

    def c_mate(slot):
        return remote(
            r.c_part.at[turn(y + slot) * 2 + 1 - core], r.c_pair.at[slot],
            r.cm_out.at[slot], r.cm_in.at[slot], mate,
        )

    def channel_norm():
        loads["cg"].wait()
        loads["ow"].wait()
        bulk(r.stats.at[pl.ds(1, NT - 1)], r.stat_sem).wait()
        total = r.stats[0]
        for j in range(1, NT):
            total = total + r.stats[j]
        average = total[0:1] / g.CH
        scale = lax.rsqrt(total[1:2] / g.CH - average * average + 1e-5)
        line = iota((8, T), 0)
        both = jnp.where(line == 0, average, jnp.where(line == 1, scale, 0.0))
        line = iota((8, F), 0)
        high = lax.Precision.HIGHEST
        average = dot(both, jnp.where(line == 0, 1.0, 0.0), 0, 0, high)
        scale = dot(both, jnp.where(line == 1, 1.0, 0.0), 0, 0, high)
        act = silu((r.mixed[...] - average) * scale * r.v_cg[...]).astype(BF)
        for j in range(NT):
            r.c_part[j] = dot(act, r.v_ow[:, j * F : (j + 1) * F]).astype(BF)
        for slot in range(Y):
            c_mate(slot).start()

    def c_sum(slot):
        c_mate(slot).wait_recv()
        mine_part = r.c_part[turn(y + slot) * 2 + core].astype(F32)
        return mine_part + r.c_pair[slot].astype(F32)

    def c_link(slot, to_slot, step):
        return remote(
            r.c_stage.at[slot], r.c_got.at[to_slot], r.c_out.at[to_slot], r.c_in.at[to_slot], tp_of(step)
        )

    def c_step(k, sign):
        slot = turn(sign * k * way)
        last = 0 if sign > 0 else Y
        to_slot = last if k == 1 else turn(sign * (k - 1) * way)
        part = c_sum(slot)
        if k < (H if sign > 0 else H - 1):
            c_link(slot, slot, 0).wait_recv()
            part = part + r.c_got[slot].astype(F32)
        r.c_stage[slot] = part.astype(BF)
        c_link(slot, to_slot, sign * way).start()

    def c_both(k):
        c_step(k, 1)
        if k < H:
            c_step(k, -1)

    TILE = S // g.TILES

    def experts_in(slot, first):
        to_mate(slot).wait_recv()
        cols = pl.ds(pl.multiple_of(turn(y + slot) * 2 * F, 2 * F), 2 * F)
        wg, wu = r.v_eg[:, cols], r.v_eu[:, cols]
        for i in range(g.TILES):
            part = pl.ds(i * TILE, TILE)
            lhs = r.ag[slot, part, :]
            a, b = dot(lhs, wg, 1, 1), dot(lhs, wu, 1, 1)
            r.gate[part, :] = a if first else r.gate[part, :] + a
            r.up[part, :] = b if first else r.up[part, :] + b

    steps = list(range(H, 0, -1))
    waiting = [0]
    for k in range(1, LA + 1):
        down, up = turn(-k * way), turn(k * way)
        for piece in range(4):
            pass_on(0, down, piece, way).wait_recv()
            if k < LA:
                pass_on(down, turn(-(k + 1) * way), piece, way).start()
            if k <= LB:
                pass_on(0, up, piece, -way).wait_recv()
                if k < LB:
                    pass_on(up, turn((k + 1) * way), piece, -way).start()
        to_mate(down).start()
        if k <= LB:
            to_mate(up).start()
        if k == 1:
            loads["eg"].wait()
            loads["eu"].wait()
        for slot in waiting:
            experts_in(slot, k == 1)
        waiting = [down, up] if k <= LB else [down]
        if k == 1:
            convolve()
        elif k == 2:
            channel_norm()
        else:
            c_both(steps.pop(0))
    if LA < 2:
        if LA < 1:
            convolve()
        channel_norm()
    if DN:
        bulk(r.ag.at[pl.ds(near, DN), pl.ds(MAIN, M - MAIN), mine], r.a2a_sem.at[3]).wait()
        bulk(r.recv_ext.at[pl.ds(1, DN), pl.ds(1, EX - 1)], r.a2a_sem.at[4]).wait()
        for i in range(DN):
            settle_ext(1 + i, near + i)
            to_mate(near + i).start()
        for slot in waiting:
            experts_in(slot, False)
        waiting = [near + i for i in range(DN)]
    for slot in waiting:
        experts_in(slot, False)
    r.hidden[...] = (silu(r.gate[...]) * r.up[...]).astype(BF)
    loads["ed"].wait()

    def m_mate(slot, piece):
        part = slice(None) if piece is None else pieces[piece]
        n = 0 if piece is None else piece
        return remote(
            r.m_full.at[slot, part, other], r.m_pair.at[slot, part, :],
            r.mm_out.at[slot, n], r.mm_in.at[slot, n], mate,
        )

    def produce(slot):
        cols = pl.ds(pl.multiple_of(turn(y + slot) * 2 * F, 2 * F), 2 * F)
        r.m_full[slot] = dot(r.hidden[...], r.v_ed[:, cols]).astype(BF)
        m_mate(slot, None).start()

    def m_link(slot, to_slot, piece, step):
        return remote(
            r.m_stage.at[slot, pieces[piece], :], r.m_got.at[to_slot, pieces[piece], :],
            r.m_out.at[to_slot, piece], r.m_in.at[to_slot, piece], tp_of(step),
        )

    def pair_sum(slot, piece):
        part = pieces[piece]
        return r.m_full[slot, part, mine].astype(F32) + r.m_pair[slot, part, :].astype(F32)

    def m_step(k, sign, piece):
        slot = turn(sign * k * way)
        last = 0 if sign > 0 else Y
        to_slot = last if k == 1 else turn(sign * (k - 1) * way)
        part = pieces[piece]
        total = pair_sum(slot, piece)
        if k < (H if sign > 0 else H - 1):
            m_link(slot, slot, piece, 0).wait_recv()
            total = total + r.m_got[slot, part, :].astype(F32)
        r.m_stage[slot, part, :] = total.astype(BF)
        m_link(slot, to_slot, piece, sign * way).start()

    far = H
    cols = pl.ds(pl.multiple_of(turn(y + far) * 2 * F, 2 * F), 2 * F)
    for piece in (3, 2, 1, 0):
        part = pieces[piece]
        r.m_full[far, part, :] = dot(r.hidden[part, :], r.v_ed[:, cols]).astype(BF)
        m_mate(far, piece).start()
    for k in range(H - 1, 0, -1):
        if k == H - 1:
            for slot in (turn(-k * way), turn(k * way)):
                produce(slot)
            for piece in (3, 2, 1, 0):
                m_mate(far, piece).wait_recv()
                m_step(H, 1, piece)
            while len(steps) > 2:
                c_both(steps.pop(0))
        m_mate(turn(-k * way), None).wait_recv()
        if k == H - 1:
            for piece in (3, 2, 1, 0):
                m_step(k, -1, piece)
        for slot in (turn(-(k - 1) * way), turn((k - 1) * way)) if k > 1 else (0,):
            produce(slot)
        if k < H - 1 and steps:
            c_both(steps.pop(0))
        m_mate(turn(k * way), None).wait_recv()
        for piece in (3, 2, 1, 0):
            m_step(k, 1, piece)
            if k < H - 1:
                m_step(k, -1, piece)

    m_mate(0, None).wait_recv()
    for piece in (3, 2, 1, 0):
        part = pieces[piece]
        total = pair_sum(0, piece)
        m_link(0, 0, piece, 0).wait_recv()
        total = total + r.m_got[0, part, :].astype(F32)
        m_link(0, Y, piece, 0).wait_recv()
        total = total + r.m_got[Y, part, :].astype(F32)
        r.back[part, :] = total.astype(BF)
        if piece == 3:
            r.rows_ext[...] = total[M - cuts[3] :]
            for b in range(EX):
                r.back_ext[b] = r.rows_ext[b * EXT : (b + 1) * EXT, :].astype(BF)
            for b in range(EX - 1, 0, -1):
                remote(
                    r.back_ext.at[b], r.home_ext.at[opposite(b)],
                    r.out_sem.at[7], r.home_sem.at[1], peer(b),
                ).start()
        for b in range(EX * (piece + 1) // 4 - 1, max(EX * piece // 4, 1) - 1, -1):
            remote(
                r.back.at[pl.ds(b * MAIN, MAIN), :], r.home.at[pl.ds(opposite(b) * MAIN, MAIN), :],
                r.out_sem.at[6], r.home_sem.at[0], peer(b),
            ).start()
    r.home[0:MAIN, :] = r.back[0:MAIN, :]
    r.home_ext[0] = r.back_ext[0]

    while steps:
        c_both(steps.pop(0))
    total = c_sum(0)
    c_link(0, 0, 0).wait_recv()
    total = total + r.c_got[0].astype(F32)
    c_link(0, Y, 0).wait_recv()
    total = total + r.c_got[Y].astype(F32)
    r.conv_out[...] = jnp.transpose(total).astype(BF)

    bulk(r.home_ext.at[pl.ds(1, EX - 1)], r.home_sem.at[1]).wait()
    for b in range(EX):
        r.rows_ext[b * EXT : (b + 1) * EXT, :] = r.home_ext[b].astype(F32)
    r.home[M:S, :] = r.rows_ext[...].astype(BF)
    bulk(r.home.at[pl.ds(MAIN, M - MAIN), :], r.home_sem.at[0]).wait()
    result = dot(r.w_hi[...], r.home[...], 0, 0) + dot(r.w_lo[...], r.home[...], 0, 0)
    r.moe_out[...] = result.astype(BF)

    bulk(r.send_main.at[0, pl.ds(MAIN, M - MAIN), :], r.out_sem.at[0]).wait()
    bulk(r.send_ext.at[0, pl.ds(1, EX - 1)], r.out_sem.at[1]).wait()
    if DN:
        bulk(r.send_main.at[pl.ds(1, DN), pl.ds(MAIN, M - MAIN), :], r.out_sem.at[2]).wait()
        bulk(r.send_ext.at[pl.ds(1, DN), pl.ds(1, EX - 1)], r.out_sem.at[3]).wait()
    halo.wait_send()
    bulk(r.stats.at[pl.ds(1, NT - 1)], r.out_sem.at[5]).wait()
    bulk(r.back.at[pl.ds(MAIN, M - MAIN), :], r.out_sem.at[6]).wait()
    bulk(r.back_ext.at[pl.ds(1, EX - 1)], r.out_sem.at[7]).wait()
    for slot in range(Y):
        to_mate(slot).wait_send()
        c_mate(slot).wait_send()
        if slot == far:
            for piece in range(4):
                m_mate(slot, piece).wait_send()
        else:
            m_mate(slot, None).wait_send()
    passed = [turn(-k * way) for k in range(1, LA + 1)] + [turn(k * way) for k in range(1, LB + 1)]
    for slot in passed:
        for piece in range(4):
            pass_on(0, slot, piece, 0).wait_send()
    final = [0, Y] + [turn(k * way) for k in range(1, H)] + [turn(-k * way) for k in range(1, H - 1)]
    for slot in final:
        c_link(0, slot, 0).wait_send()
        for piece in range(4):
            m_link(0, slot, piece, 0).wait_send()


def run(Z, X, args):
    (tok_a, gain_a, vw, gw, ker, cg, ow, tok_b, gain_b, routes, logits, eg, eu, ed) = args
    EX, NT = lax.axis_size("ep"), lax.axis_size("tp")
    T, D = tok_a.shape
    R, F, HU = tok_b.shape[0], vw.shape[1], eg.shape[2]
    cap = 3 * R * routes.shape[1] // (2 * EX)
    EXT, Y, DN = cap - MAIN, NT // 2, 2
    S, M = EX * cap, EX * MAIN
    given = dict(
        tok_b=tok_b, routes=routes.T, logits=logits.T, gain_b=gain_b.reshape(NT, F),
        tok_a=tok_a, gain_a=gain_a.reshape(NT, F), vw=vw, gw=gw, ker=ker, cg=cg.reshape(1, F),
        ow=ow, eg=eg[0].T, eu=eu[0].T, ed=ed[0],
    )
    vm, dma = pltpu.VMEM, pltpu.SemaphoreType.DMA
    scratch = dict(
        {"v_" + n: vm(given[n].shape, given[n].dtype) for n in INPUTS},
        in_sem=dma((len(INPUTS),)), w_hi=vm((S, R), BF), w_lo=vm((S, R), BF),
        send_main=vm((DN + 1, M, F), BF), send_ext=vm((DN + 1, EX, EXT, F), BF),
        recv_ext=vm((DN + 1, EX, EXT, F), BF),
        rows_ext=vm((EX * EXT, F), F32), ag=vm((Y, S, 2 * F), BF),
        out_sem=dma((8,)), a2a_sem=dma((5,)), normed_a=vm((T, D), BF), padded=vm((T + 32, F), F32),
        tail=vm((32, F), BF), halo=vm((32, F), BF), halo_sem=dma, mixed=vm((T, F), F32),
        stats=vm((NT, 2, T), F32), stat_sem=dma,
        ag_out=dma((Y, 4)), ag_in=dma((Y, 4)), am_out=dma((Y,)), am_in=dma((Y,)),
        c_part=vm((NT, T, F), BF), c_pair=vm((Y, T, F), BF), c_stage=vm((Y, T, F), BF),
        c_got=vm((Y + 1, T, F), BF), cm_out=dma((Y,)), cm_in=dma((Y,)), c_out=dma((Y + 1,)),
        c_in=dma((Y + 1,)), gate=vm((S, HU), F32), up=vm((S, HU), F32), hidden=vm((S, HU), BF),
        m_full=vm((Y, S, 2 * F), BF), m_pair=vm((Y, S, F), BF), m_stage=vm((Y, S, F), BF),
        m_got=vm((Y + 1, S, F), BF), mm_out=dma((Y, 4)), mm_in=dma((Y, 4)), m_out=dma((Y + 1, 4)),
        m_in=dma((Y + 1, 4)), back=vm((S, F), BF), back_ext=vm((EX, EXT, F), BF),
        home=vm((S, F), BF), home_ext=vm((EX, EXT, F), BF), home_sem=dma((2,)),
    )
    names = ["in_" + n for n in INPUTS] + ["conv_out", "moe_out"] + list(scratch)
    g = SimpleNamespace(
        names=names, Z=Z, X=X, Y=Y, F=F, EX=EX, EXT=EXT, NT=NT, T=T, R=R, D=D, S=S, CH=NT * F,
        TAPS=ker.shape[0], TILES=3, DN=DN,
    )
    conv_out, moe_out = pl.pallas_call(
        functools.partial(kernel, g),
        out_shape=(pltpu.VMEM((F, T), BF), pltpu.VMEM((R, F), BF)),
        in_specs=[pl.BlockSpec(memory_space=pl.ANY)] * len(INPUTS),
        out_specs=(pl.BlockSpec(memory_space=pltpu.VMEM),) * 2,
        scratch_shapes=list(scratch.values()),
        compiler_params=pltpu.CompilerParams(
            collective_id=0, has_side_effects=True, vmem_limit_bytes=60 * 1024 * 1024
        ),
    )(*[given[n] for n in INPUTS])
    return conv_out, moe_out.T


def solution(mesh, Z=8, X=4):
    return jax.shard_map(
        lambda *args: run(Z, X, args),
        mesh=mesh,
        in_specs=(
            P("ep", None), P(), P(None, "tp"), P(None, "tp"), P(None, "tp"), P("tp"), P("tp", None),
            P("ep", None), P(), P("ep", None), P("ep", None), P("ep", None, "tp"),
            P("ep", None, "tp"), P("ep", "tp", None),
        ),
        out_specs=(P("tp", "ep"), P("tp", "ep")),
        check_vma=False,
    )
```

```python
import functools
from types import SimpleNamespace

import jax
import jax.numpy as jnp
from jax import lax
from jax.experimental import pallas as pl
from jax.experimental.pallas import tpu as pltpu
from jax.sharding import PartitionSpec as P

MESH = pl.DeviceIdType.MESH
BF = jnp.bfloat16
F32 = jnp.float32
I32 = jnp.int32
MAIN = 16
INPUTS = (
    "routes", "logits", "tok_b", "gain_b", "tok_a", "gain_a", "vw", "gw",
    "ker", "cg", "ow", "eg", "eu", "ed",
)


def iota(shape, dim):
    return lax.broadcasted_iota(I32, shape, dim)


def dot(a, b, ca=1, cb=0, precision=None):
    return lax.dot_general(
        a, b, (((ca,), (cb,)), ((), ())), precision=precision, preferred_element_type=F32
    )


def silu(v):
    return v / (1.0 + jnp.exp(-v))


def kernel(g, *refs):
    r = SimpleNamespace(**dict(zip(g.names, refs)))
    Z, X, Y, F, EX, EXT = g.Z, g.X, g.Y, g.F, g.EX, g.EXT
    NT, T, R, D, S = g.NT, g.T, g.R, g.D, g.S
    M = EX * MAIN
    HALF = M // 2
    H, DN = Y // 2, g.DN
    LA, LB = H - (DN + 1) // 2, H - 1 - DN // 2
    e = lax.axis_index("ep")
    t = lax.axis_index("tp")
    core, y = lax.rem(t, 2), lax.div(t, 2)
    z, x = lax.div(e, X), lax.rem(e, X)
    way = 1 - 2 * core
    mate = (e, t + way)
    mine = pl.ds(pl.multiple_of(core * F, F), F)
    other = pl.ds(pl.multiple_of((1 - core) * F, F), F)
    near = H - 1 + core if DN == 2 else H - DN // 2

    def turn(a):
        return lax.rem(a + 4 * Y, Y)

    def tp_of(step):
        return (e, turn(y + step) * 2 + core)

    def place(b):
        i, dx = b // X, b % X
        dz = jnp.where(i % 2 == 1, (i + 1) // 2, Z - i // 2)
        return lax.rem(z + dz, Z) * X + lax.rem(x + dx, X)

    rows_of = [lax.rem(z + i, Z) * X for i in range(Z)]
    cols_of = [lax.rem(x + i, X) for i in range(X)]

    def peer(b):
        i, dx = divmod(b, X)
        dz = ((i + 1) // 2 if i % 2 else Z - i // 2) % Z
        return (rows_of[dz] + cols_of[dx], t)

    def opposite(b):
        i, dx = divmod(b, X)
        back = i if i in (0, Z - 1) else (i + 1 if i % 2 else i - 1)
        return back * X + (X - dx) % X

    def remote(src, dst, send, recv, to):
        return pltpu.make_async_remote_copy(
            src_ref=src, dst_ref=dst, send_sem=send, recv_sem=recv, device_id=to, device_id_type=MESH
        )

    loads = {}
    for i, name in enumerate(INPUTS):
        loads[name] = pltpu.make_async_copy(
            getattr(r, "in_" + name), getattr(r, "v_" + name), r.in_sem.at[i]
        )
    for name in INPUTS[:4]:
        loads[name].start()

    barrier = pltpu.get_barrier_semaphore()

    for b in range(EX - 1, 0, -1):
        pl.semaphore_signal(barrier, 1, device_id=peer(b), device_id_type=MESH)
    tps = [(e, lax.rem(t + i, NT)) for i in range(NT)]
    for i in range(1, NT):
        pl.semaphore_signal(barrier, 1, device_id=tps[i], device_id_type=MESH)
    for name in INPUTS[4:]:
        loads[name].start()

    s = iota((1, S), 1)
    block = jnp.where(s < M, s // MAIN, (s - M) // EXT)
    rank = jnp.where(s < M, s % MAIN, MAIN + (s - M) % EXT) + 1
    line = iota((EX + 8, S), 0)
    spread = jnp.where(line == place(block), 1.0, jnp.where(line == EX, rank.astype(F32), 0.0))
    r.spread[...] = spread.astype(BF)
    for name in ("routes", "logits"):
        loads[name].wait()
    lines = iota((EX, R), 0)
    first = jnp.where(lines == r.v_routes[0:1, :], 1.0, 0.0)
    second = jnp.where(lines == r.v_routes[1:2, :], 1.0, 0.0)
    named = first + second
    earlier = jnp.where(iota((R, R), 0) < iota((R, R), 1), 1.0, 0.0).astype(BF)
    r.code[0:EX, :] = named * (dot(named.astype(BF), earlier) + 1.0)
    r.code[EX:, :] = jnp.where(iota((8, R), 0) == 0, -1.0, 0.0)
    l0, l1 = r.v_logits[0:1, :], r.v_logits[1:2, :]
    top = jnp.maximum(l0, l1)
    e0, e1 = jnp.exp(l0 - top), jnp.exp(l1 - top)
    weight = first * (e0 / (e0 + e1)) + second * (e1 / (e0 + e1))
    r.weight[...] = weight

    for name in ("tok_b", "gain_b"):
        loads[name].wait()
    squares = jnp.zeros((R, F), F32)
    for j in range(NT):
        v = r.v_tok_b[:, j * F : (j + 1) * F].astype(F32)
        squares = squares + v * v
    inv = lax.rsqrt(jnp.sum(squares, axis=1, keepdims=True) / D + 1e-6)

    lag = dot(r.spread[...], r.code[...].astype(BF), 0, 0)
    r.picks[...] = jnp.where(lag == 0.0, 1.0, 0.0).astype(BF)

    def rows_for(i, slot):
        col = turn(y + slot) * 2 + core
        own = r.v_tok_b[:, pl.ds(pl.multiple_of(col * F, F), F)].astype(F32)
        normed = (own * inv * r.v_gain_b[pl.ds(col, 1), :]).astype(BF)
        rows = dot(r.picks[...], normed)
        r.send_main[i] = rows[:M].astype(BF)
        r.ag[slot, 0:MAIN, mine] = rows[:MAIN].astype(BF)
        r.rows_ext[...] = rows[M:]
        for b in range(EX):
            r.send_ext[i, b] = r.rows_ext[b * EXT : (b + 1) * EXT, :].astype(BF)
        r.recv_ext[i, 0] = r.rows_ext[0:EXT, :].astype(BF)

    rows_for(0, 0)
    pl.semaphore_wait(barrier, EX - 1 + NT - 1)
    for b in range(1, EX):
        nb = opposite(b)
        remote(
            r.send_main.at[0, pl.ds(b * MAIN, MAIN), :], r.ag.at[0, pl.ds(nb * MAIN, MAIN), mine],
            r.out_sem.at[0], r.a2a_sem.at[nb // (EX // 2)], peer(b),
        ).start()
        remote(
            r.send_ext.at[0, b], r.recv_ext.at[0, nb], r.out_sem.at[1], r.a2a_sem.at[2], peer(b)
        ).start()

    for name in ("tok_a", "gain_a", "vw", "gw"):
        loads[name].wait()
    squares = jnp.zeros((T, F), F32)
    for j in range(NT):
        v = r.v_tok_a[:, j * F : (j + 1) * F].astype(F32)
        squares = squares + v * v
    inv_a = lax.rsqrt(jnp.sum(squares, axis=1, keepdims=True) / D + 1e-6)
    for j in range(NT):
        cols = slice(j * F, (j + 1) * F)
        v = r.v_tok_a[:, cols].astype(F32) * inv_a * r.v_gain_a[j : j + 1, :]
        r.normed_a[:, cols] = v.astype(BF)
    value = dot(r.normed_a[...], r.v_vw[...])
    gate = dot(r.normed_a[...], r.v_gw[...])
    glu = (value / (1.0 + jnp.exp(-gate))).astype(BF)
    r.padded[32:, :] = glu.astype(F32)
    r.tail[...] = glu[T - 32 :, :]
    halo = remote(r.tail, r.halo, r.out_sem.at[4], r.halo_sem, (lax.rem(e + 1, EX), t))
    halo.start()

    for i in range(DN):
        rows_for(1 + i, near + i)
    for b in range(1, EX if DN else 0):
        nb = opposite(b)
        remote(
            r.send_main.at[pl.ds(1, DN), pl.ds(b * MAIN, MAIN), :],
            r.ag.at[pl.ds(near, DN), pl.ds(nb * MAIN, MAIN), mine],
            r.out_sem.at[2], r.a2a_sem.at[3], peer(b),
        ).start()
        remote(
            r.send_ext.at[pl.ds(1, DN), b], r.recv_ext.at[pl.ds(1, DN), nb],
            r.out_sem.at[3], r.a2a_sem.at[4], peer(b),
        ).start()
    weight = r.weight[...]
    w_hi = weight.astype(BF)
    w_lo = (weight - w_hi.astype(F32)).astype(BF)
    r.w_hi[...] = (r.picks[...].astype(F32) * dot(r.spread[0:EX, :], w_hi, 0, 0)).astype(BF)
    r.w_lo[...] = (r.picks[...].astype(F32) * dot(r.spread[0:EX, :], w_lo, 0, 0)).astype(BF)

    cuts = [(EX * i // 4) * MAIN for i in range(4)] + [S]
    pieces = [pl.ds(a, b - a) for a, b in zip(cuts, cuts[1:])]

    def pass_on(sign, k, piece):
        return remote(
            r.ag.at[turn(-sign * (k - 1) * way), pieces[piece], mine],
            r.ag.at[turn(-sign * k * way), pieces[piece], mine],
            r.out_sem.at[8], r.ag_in.at[k - 1 if sign > 0 else LA + k - 1, piece], tp_of(sign * way),
        )

    def to_mate(slot):
        return remote(
            r.ag.at[slot, :, mine], r.ag.at[slot, :, mine], r.out_sem.at[9], r.am_in.at[slot], mate
        )

    def bulk(ref, sem):
        return pltpu.make_async_copy(ref, ref, sem)

    def settle_ext(i, slot):
        for b in range(EX):
            r.rows_ext[b * EXT : (b + 1) * EXT, :] = r.recv_ext[i, b].astype(F32)
        r.ag[slot, M:S, mine] = r.rows_ext[...].astype(BF)

    def convolve():
        loads["ker"].wait()
        halo.wait_recv()
        r.padded[0:32, :] = jnp.where(e > 0, r.halo[...].astype(F32), 0.0)
        mixed = jnp.zeros((T, F), F32)
        for tap in range(g.TAPS):
            low = 32 - (g.TAPS - 1) + tap
            mixed = mixed + r.v_ker[tap : tap + 1, :] * r.padded[low : low + T, :]
        r.mixed[...] = mixed
        ones = jnp.ones((8, F), F32)
        sums = dot(ones, mixed, 1, 1, lax.Precision.HIGHEST)
        powers = dot(ones, mixed * mixed, 1, 1, lax.Precision.HIGHEST)
        r.stats[0] = jnp.where(iota((8, T), 0) == 0, sums, powers)[0:2]

        for i in range(1, NT):
            remote(
                r.stats.at[0], r.stats.at[NT - i], r.out_sem.at[5], r.stat_sem, tps[i]
            ).start()

    bulk(r.ag.at[0, pl.ds(MAIN, HALF - MAIN), mine], r.a2a_sem.at[0]).wait()
    for piece in (0, 1):
        if LA:
            pass_on(1, 1, piece).start()
        if LB:
            pass_on(-1, 1, piece).start()
    convolve()
    bulk(r.ag.at[0, pl.ds(HALF, HALF), mine], r.a2a_sem.at[1]).wait()
    bulk(r.recv_ext.at[0, pl.ds(1, EX - 1)], r.a2a_sem.at[2]).wait()
    settle_ext(0, 0)
    for piece in (2, 3):
        if LA:
            pass_on(1, 1, piece).start()
        if LB:
            pass_on(-1, 1, piece).start()
    to_mate(0).start()

    def c_mate(slot):
        return remote(
            r.c_part.at[turn(y + slot) * 2 + 1 - core], r.c_pair.at[slot],
            r.out_sem.at[10], r.cm_in, mate,
        )

    def channel_norm():
        loads["cg"].wait()
        loads["ow"].wait()
        bulk(r.stats.at[pl.ds(1, NT - 1)], r.stat_sem).wait()
        total = r.stats[0]
        for j in range(1, NT):
            total = total + r.stats[j]
        average = total[0:1] / g.CH
        scale = lax.rsqrt(total[1:2] / g.CH - average * average + 1e-5)
        line = iota((8, T), 0)
        both = jnp.where(line == 0, average, jnp.where(line == 1, scale, 0.0))
        line = iota((8, F), 0)
        high = lax.Precision.HIGHEST
        average = dot(both, jnp.where(line == 0, 1.0, 0.0), 0, 0, high)
        scale = dot(both, jnp.where(line == 1, 1.0, 0.0), 0, 0, high)
        act = silu((r.mixed[...] - average) * scale * r.v_cg[...]).astype(BF)
        for j in range(NT):
            r.c_part[j] = dot(act, r.v_ow[:, j * F : (j + 1) * F]).astype(BF)
        for slot in range(Y):
            c_mate(slot).start()

    def c_sum(slot):
        mine_part = r.c_part[turn(y + slot) * 2 + core].astype(F32)
        return mine_part + r.c_pair[slot].astype(F32)

    def hop(k, sign):
        return H - k if sign > 0 else 2 * H - 1 - k

    def c_link(k, sign):
        n = hop(k, sign)
        return remote(
            r.c_stage.at[n], r.c_got.at[n], r.out_sem.at[11], r.c_in.at[n], tp_of(sign * way)
        )

    def c_step(k, sign):
        part = c_sum(turn(sign * k * way))
        if k < (H if sign > 0 else H - 1):
            c_link(k + 1, sign).wait_recv()
            part = part + r.c_got[hop(k + 1, sign)].astype(F32)
        r.c_stage[hop(k, sign)] = part.astype(BF)
        c_link(k, sign).start()

    def c_both(k):
        if k == H:
            bulk(r.c_pair, r.cm_in).wait()
        c_step(k, 1)
        if k < H:
            c_step(k, -1)

    TILE = S // g.TILES

    def experts_in(slot, first):
        to_mate(slot).wait_recv()
        cols = pl.ds(pl.multiple_of(turn(y + slot) * 2 * F, 2 * F), 2 * F)
        wg, wu = r.v_eg[:, cols], r.v_eu[:, cols]
        for i in range(g.TILES):
            part = pl.ds(i * TILE, TILE)
            lhs = r.ag[slot, part, :]
            a, b = dot(lhs, wg, 1, 1), dot(lhs, wu, 1, 1)
            r.gate[part, :] = a if first else r.gate[part, :] + a
            r.up[part, :] = b if first else r.up[part, :] + b

    loads["eg"].wait()
    loads["eu"].wait()
    steps = list(range(H, 0, -1))
    waiting = [0]

    def take_direct():
        bulk(r.ag.at[pl.ds(near, DN), pl.ds(MAIN, M - MAIN), mine], r.a2a_sem.at[3]).wait()
        bulk(r.recv_ext.at[pl.ds(1, DN), pl.ds(1, EX - 1)], r.a2a_sem.at[4]).wait()
        for i in range(DN):
            settle_ext(1 + i, near + i)
            to_mate(near + i).start()
        return [H] if DN == 2 else [near + i for i in range(DN)]

    for k in range(1, LA + 1):
        if DN and k == g.DIRECT_AT:
            waiting = waiting + take_direct()
        down, up = turn(-k * way), turn(k * way)
        for piece in range(4):
            pass_on(1, k, piece).wait_recv()
            if k < LA:
                pass_on(1, k + 1, piece).start()
            if k <= LB:
                pass_on(-1, k, piece).wait_recv()
                if k < LB:
                    pass_on(-1, k + 1, piece).start()
        to_mate(down).start()
        if k <= LB:
            to_mate(up).start()
        for i, slot in enumerate(waiting):
            experts_in(slot, k == 1 and i == 0)
        waiting = [up, down] if k <= LB else [down]
        if k == 1:
            channel_norm()
        elif k == 2:
            c_both(steps.pop(0))
    c_both(steps.pop(0))
    if DN == 2:
        waiting = waiting + [turn((H - 1) * way)]
    for slot in waiting[:-1]:
        experts_in(slot, False)
    loads["ed"].wait()
    if len(steps) > 2:
        c_both(steps.pop(0))

    def m_mate(slot, piece):
        part = slice(None) if piece is None else pieces[piece]
        return remote(
            r.m_full.at[slot, part, other], r.m_pair.at[slot, part, :],
            r.out_sem.at[12], r.mm_in.at[slot if piece is None else Y + piece], mate,
        )

    def produce(slot):
        cols = pl.ds(pl.multiple_of(turn(y + slot) * 2 * F, 2 * F), 2 * F)
        r.m_full[slot] = dot(r.hidden[...], r.v_ed[:, cols]).astype(BF)
        m_mate(slot, None).start()

    def m_link(k, sign, piece):
        n, part = hop(k, sign), pieces[piece]
        return remote(
            r.m_stage.at[n, part, :], r.m_got.at[n, part, :],
            r.out_sem.at[13], r.m_in.at[n, piece], tp_of(sign * way),
        )

    def pair_sum(slot, piece):
        part = pieces[piece]
        return r.m_full[slot, part, mine].astype(F32) + r.m_pair[slot, part, :].astype(F32)

    def m_step(k, sign, piece):
        part = pieces[piece]
        total = pair_sum(turn(sign * k * way), piece)
        if k < (H if sign > 0 else H - 1):
            m_link(k + 1, sign, piece).wait_recv()
            total = total + r.m_got[hop(k + 1, sign), part, :].astype(F32)
        r.m_stage[hop(k, sign), part, :] = total.astype(BF)
        m_link(k, sign, piece).start()

    to_mate(waiting[-1]).wait_recv()
    far = H

    def wide(slot):
        return pl.ds(pl.multiple_of(turn(y + slot) * 2 * F, 2 * F), 2 * F)

    cols = wide(waiting[-1])
    wg, wu = r.v_eg[:, cols], r.v_eu[:, cols]
    for piece in (3, 2, 1, 0):
        part = pieces[piece]
        lhs = r.ag[waiting[-1], part, :]
        a = r.gate[part, :] + dot(lhs, wg, 1, 1)
        b = r.up[part, :] + dot(lhs, wu, 1, 1)
        hidden = (silu(a) * b).astype(BF)
        r.hidden[part, :] = hidden
        r.m_full[far, part, :] = dot(hidden, r.v_ed[:, wide(far)]).astype(BF)
        m_mate(far, piece).start()
    for slot in (turn(-(H - 1) * way), turn((H - 1) * way)):
        produce(slot)
    for piece in (3, 2, 1, 0):
        m_mate(far, piece).wait_recv()
        m_step(H, 1, piece)
    if H > 1:
        m_mate(turn(-(H - 1) * way), None).wait_recv()
        for piece in (3, 2, 1, 0):
            m_step(H - 1, -1, piece)
    if H > 2:
        for slot in (turn(-(H - 2) * way), turn((H - 2) * way)):
            produce(slot)
    for k in range(H - 1, 0, -1):
        m_mate(turn(k * way), None).wait_recv()
        for piece in (3, 2, 1, 0):
            m_step(k, 1, piece)
            if k > 1:
                if piece == 3:
                    m_mate(turn(-(k - 1) * way), None).wait_recv()
                m_step(k - 1, -1, piece)
        if k > 2:
            for slot in (turn(-(k - 2) * way), turn((k - 2) * way)):
                produce(slot)
        elif k == 2 or H == 2:
            produce(0)
        if k == g.C_AT and len(steps) > 1:
            c_both(steps.pop(0))

    m_mate(0, None).wait_recv()
    for piece in (3, 2, 1, 0):
        part = pieces[piece]
        total = pair_sum(0, piece)
        for sign in (1, -1):
            m_link(1, sign, piece).wait_recv()
            total = total + r.m_got[hop(1, sign), part, :].astype(F32)
        r.back[part, :] = total.astype(BF)
        if piece == 3:
            r.rows_ext[...] = total[M - cuts[3] :]
            for b in range(EX):
                r.back_ext[b] = r.rows_ext[b * EXT : (b + 1) * EXT, :].astype(BF)
            for b in range(EX - 1, 0, -1):
                remote(
                    r.back_ext.at[b], r.home_ext.at[opposite(b)],
                    r.out_sem.at[7], r.home_sem.at[1], peer(b),
                ).start()
        for b in range(EX * (piece + 1) // 4 - 1, max(EX * piece // 4, 1) - 1, -1):
            remote(
                r.back.at[pl.ds(b * MAIN, MAIN), :], r.home.at[pl.ds(opposite(b) * MAIN, MAIN), :],
                r.out_sem.at[6], r.home_sem.at[0], peer(b),
            ).start()
    r.home[0:MAIN, :] = r.back[0:MAIN, :]
    r.home_ext[0] = r.back_ext[0]

    while steps:
        c_both(steps.pop(0))
    total = c_sum(0)
    for sign in (1, -1):
        c_link(1, sign).wait_recv()
        total = total + r.c_got[hop(1, sign)].astype(F32)
    r.conv_out[...] = jnp.transpose(total).astype(BF)

    bulk(r.home_ext.at[pl.ds(1, EX - 1)], r.home_sem.at[1]).wait()
    for b in range(EX):
        r.rows_ext[b * EXT : (b + 1) * EXT, :] = r.home_ext[b].astype(F32)
    r.home[M:S, :] = r.rows_ext[...].astype(BF)
    bulk(r.home.at[pl.ds(MAIN, M - MAIN), :], r.home_sem.at[0]).wait()
    result = dot(r.w_hi[...], r.home[...], 0, 0) + dot(r.w_lo[...], r.home[...], 0, 0)
    r.moe_out[...] = result.astype(BF)

    bulk(r.send_main.at[0, pl.ds(MAIN, M - MAIN), :], r.out_sem.at[0]).wait()
    bulk(r.send_ext.at[0, pl.ds(1, EX - 1)], r.out_sem.at[1]).wait()
    if DN:
        bulk(r.send_main.at[pl.ds(1, DN), pl.ds(MAIN, M - MAIN), :], r.out_sem.at[2]).wait()
        bulk(r.send_ext.at[pl.ds(1, DN), pl.ds(1, EX - 1)], r.out_sem.at[3]).wait()
    halo.wait_send()
    bulk(r.stats.at[pl.ds(1, NT - 1)], r.out_sem.at[5]).wait()
    bulk(r.back.at[pl.ds(MAIN, M - MAIN), :], r.out_sem.at[6]).wait()
    bulk(r.back_ext.at[pl.ds(1, EX - 1)], r.out_sem.at[7]).wait()
    if LA + LB:
        bulk(r.ag.at[pl.ds(0, LA + LB), :, mine], r.out_sem.at[8]).wait()
    bulk(r.ag.at[:, :, mine], r.out_sem.at[9]).wait()
    bulk(r.c_part.at[pl.ds(0, Y)], r.out_sem.at[10]).wait()
    bulk(r.c_stage, r.out_sem.at[11]).wait()
    bulk(r.m_full.at[:, :, other], r.out_sem.at[12]).wait()
    bulk(r.m_stage, r.out_sem.at[13]).wait()


def run(Z, X, args):
    (tok_a, gain_a, vw, gw, ker, cg, ow, tok_b, gain_b, routes, logits, eg, eu, ed) = args
    EX, NT = lax.axis_size("ep"), lax.axis_size("tp")
    T, D = tok_a.shape
    R, F, HU = tok_b.shape[0], vw.shape[1], eg.shape[2]
    cap = 3 * R * routes.shape[1] // (2 * EX)
    EXT, Y, DN = cap - MAIN, NT // 2, 2
    S, M = EX * cap, EX * MAIN
    given = dict(
        tok_b=tok_b, routes=routes.T, logits=logits.T, gain_b=gain_b.reshape(NT, F),
        tok_a=tok_a, gain_a=gain_a.reshape(NT, F), vw=vw, gw=gw, ker=ker, cg=cg.reshape(1, F),
        ow=ow, eg=eg[0].T, eu=eu[0].T, ed=ed[0],
    )
    vm, dma = pltpu.VMEM, pltpu.SemaphoreType.DMA
    scratch = dict(
        {"v_" + n: vm(given[n].shape, given[n].dtype) for n in INPUTS},
        in_sem=dma((len(INPUTS),)), spread=vm((EX + 8, S), BF), code=vm((EX + 8, R), F32),
        picks=vm((S, R), BF), weight=vm((EX, R), F32), w_hi=vm((S, R), BF), w_lo=vm((S, R), BF),
        send_main=vm((DN + 1, M, F), BF), send_ext=vm((DN + 1, EX, EXT, F), BF),
        recv_ext=vm((DN + 1, EX, EXT, F), BF),
        rows_ext=vm((EX * EXT, F), F32), ag=vm((Y, S, 2 * F), BF),
        out_sem=dma((14,)), a2a_sem=dma((5,)), normed_a=vm((T, D), BF), padded=vm((T + 32, F), F32),
        tail=vm((32, F), BF), halo=vm((32, F), BF), halo_sem=dma, mixed=vm((T, F), F32),
        stats=vm((NT, 2, T), F32), stat_sem=dma,
        ag_in=dma((max(Y - 1 - DN, 1), 4)), am_in=dma((Y,)),
        c_part=vm((NT, T, F), BF), c_pair=vm((Y, T, F), BF), c_stage=vm((Y - 1, T, F), BF),
        c_got=vm((Y - 1, T, F), BF), cm_in=dma, c_in=dma((Y - 1,)),
        gate=vm((S, HU), F32), up=vm((S, HU), F32), hidden=vm((S, HU), BF),
        m_full=vm((Y, S, 2 * F), BF), m_pair=vm((Y, S, F), BF), m_stage=vm((Y - 1, S, F), BF),
        m_got=vm((Y - 1, S, F), BF), mm_in=dma((Y + 4,)), m_in=dma((Y - 1, 4)), back=vm((S, F), BF), back_ext=vm((EX, EXT, F), BF),
        home=vm((S, F), BF), home_ext=vm((EX, EXT, F), BF), home_sem=dma((2,)),
    )
    names = ["in_" + n for n in INPUTS] + ["conv_out", "moe_out"] + list(scratch)
    g = SimpleNamespace(
        names=names, Z=Z, X=X, Y=Y, F=F, EX=EX, EXT=EXT, NT=NT, T=T, R=R, D=D, S=S, CH=NT * F,
        TAPS=ker.shape[0], TILES=3, DN=DN, DIRECT_AT=max(NT // 4 - (DN + 1) // 2, 1), C_AT=2,
    )
    conv_out, moe_out = pl.pallas_call(
        functools.partial(kernel, g),
        out_shape=(pltpu.VMEM((F, T), BF), pltpu.VMEM((R, F), BF)),
        in_specs=[pl.BlockSpec(memory_space=pl.ANY)] * len(INPUTS),
        out_specs=(pl.BlockSpec(memory_space=pltpu.VMEM),) * 2,
        scratch_shapes=list(scratch.values()),
        compiler_params=pltpu.CompilerParams(
            collective_id=0, has_side_effects=True, vmem_limit_bytes=60 * 1024 * 1024
        ),
    )(*[given[n] for n in INPUTS])
    return conv_out, moe_out.T


def solution(mesh, Z=8, X=4):
    return jax.shard_map(
        lambda *args: run(Z, X, args),
        mesh=mesh,
        in_specs=(
            P("ep", None), P(), P(None, "tp"), P(None, "tp"), P(None, "tp"), P("tp"), P("tp", None),
            P("ep", None), P(), P("ep", None), P("ep", None), P("ep", None, "tp"),
            P("ep", None, "tp"), P("ep", "tp", None),
        ),
        out_specs=(P("tp", "ep"), P("tp", "ep")),
        check_vma=False,
    )
```

```python
import functools
from types import SimpleNamespace

import jax
import jax.numpy as jnp
from jax import lax
from jax.experimental import pallas as pl
from jax.experimental.pallas import tpu as pltpu
from jax.sharding import PartitionSpec as P

MESH = pl.DeviceIdType.MESH
BF = jnp.bfloat16
F32 = jnp.float32
I32 = jnp.int32
MAIN = 16
INPUTS = (
    "routes", "logits", "tok_b", "gain_b", "tok_a", "gain_a", "vw", "gw",
    "ker", "cg", "ow", "eg", "eu", "ed",
)


def iota(shape, dim):
    return lax.broadcasted_iota(I32, shape, dim)


def dot(a, b, ca=1, cb=0, precision=None):
    return lax.dot_general(
        a, b, (((ca,), (cb,)), ((), ())), precision=precision, preferred_element_type=F32
    )


def silu(v):
    return v / (1.0 + jnp.exp(-v))


def kernel(g, *refs):
    r = SimpleNamespace(**dict(zip(g.names, refs)))
    Z, X, Y, F, EX, EXT = g.Z, g.X, g.Y, g.F, g.EX, g.EXT
    NT, T, R, D, S = g.NT, g.T, g.R, g.D, g.S
    M = EX * MAIN
    HALF = M // 2
    H, DN = Y // 2, g.DN
    LA, LB = H - (DN + 1) // 2, H - 1 - DN // 2
    e = lax.axis_index("ep")
    t = lax.axis_index("tp")
    core, y = lax.rem(t, 2), lax.div(t, 2)
    z, x = lax.div(e, X), lax.rem(e, X)
    way = 1 - 2 * core
    mate = (e, t + way)
    mine = pl.ds(pl.multiple_of(core * F, F), F)
    other = pl.ds(pl.multiple_of((1 - core) * F, F), F)
    near = H - 1 + core if DN == 2 else H - DN // 2

    def turn(a):
        return lax.rem(a + 4 * Y, Y)

    def tp_of(step):
        return (e, turn(y + step) * 2 + core)

    def place(b):
        i, dx = b // X, b % X
        dz = jnp.where(i % 2 == 1, (i + 1) // 2, Z - i // 2)
        return lax.rem(z + dz, Z) * X + lax.rem(x + dx, X)

    rows_of = [lax.rem(z + i, Z) * X for i in range(Z)]
    cols_of = [lax.rem(x + i, X) for i in range(X)]

    def peer(b):
        i, dx = divmod(b, X)
        dz = ((i + 1) // 2 if i % 2 else Z - i // 2) % Z
        return (rows_of[dz] + cols_of[dx], t)

    def opposite(b):
        i, dx = divmod(b, X)
        back = i if i in (0, Z - 1) else (i + 1 if i % 2 else i - 1)
        return back * X + (X - dx) % X

    def remote(src, dst, send, recv, to):
        return pltpu.make_async_remote_copy(
            src_ref=src, dst_ref=dst, send_sem=send, recv_sem=recv, device_id=to, device_id_type=MESH
        )

    loads = {}
    for i, name in enumerate(INPUTS):
        loads[name] = pltpu.make_async_copy(
            getattr(r, "in_" + name), getattr(r, "v_" + name), r.in_sem.at[i]
        )
    for name in INPUTS[:4]:
        loads[name].start()

    barrier = pltpu.get_barrier_semaphore()

    for b in range(EX - 1, 0, -1):
        pl.semaphore_signal(barrier, 1, device_id=peer(b), device_id_type=MESH)
    tps = [(e, lax.rem(t + i, NT)) for i in range(NT)]
    for i in range(1, NT):
        pl.semaphore_signal(barrier, 1, device_id=tps[i], device_id_type=MESH)
    for name in INPUTS[4:]:
        loads[name].start()

    s = iota((1, S), 1)
    block = jnp.where(s < M, s // MAIN, (s - M) // EXT)
    rank = jnp.where(s < M, s % MAIN, MAIN + (s - M) % EXT) + 1
    line = iota((EX + 8, S), 0)
    spread = jnp.where(line == place(block), 1.0, jnp.where(line == EX, rank.astype(F32), 0.0))
    r.spread[...] = spread.astype(BF)
    for name in ("routes", "logits"):
        loads[name].wait()
    lines = iota((EX, R), 0)
    first = jnp.where(lines == r.v_routes[0:1, :], 1.0, 0.0)
    second = jnp.where(lines == r.v_routes[1:2, :], 1.0, 0.0)
    named = first + second
    earlier = jnp.where(iota((R, R), 0) < iota((R, R), 1), 1.0, 0.0).astype(BF)
    r.code[0:EX, :] = named * (dot(named.astype(BF), earlier) + 1.0)
    r.code[EX:, :] = jnp.where(iota((8, R), 0) == 0, -1.0, 0.0)
    l0, l1 = r.v_logits[0:1, :], r.v_logits[1:2, :]
    top = jnp.maximum(l0, l1)
    e0, e1 = jnp.exp(l0 - top), jnp.exp(l1 - top)
    weight = first * (e0 / (e0 + e1)) + second * (e1 / (e0 + e1))
    r.weight[...] = weight

    for name in ("tok_b", "gain_b"):
        loads[name].wait()
    squares = jnp.zeros((R, F), F32)
    for j in range(NT):
        v = r.v_tok_b[:, j * F : (j + 1) * F].astype(F32)
        squares = squares + v * v
    inv = lax.rsqrt(jnp.sum(squares, axis=1, keepdims=True) / D + 1e-6)

    lag = dot(r.spread[...], r.code[...].astype(BF), 0, 0)
    r.picks[...] = jnp.where(lag == 0.0, 1.0, 0.0).astype(BF)

    def rows_for(i, slot):
        col = turn(y + slot) * 2 + core
        own = r.v_tok_b[:, pl.ds(pl.multiple_of(col * F, F), F)].astype(F32)
        normed = (own * inv * r.v_gain_b[pl.ds(col, 1), :]).astype(BF)
        rows = dot(r.picks[...], normed)
        r.send_main[i] = rows[:M].astype(BF)
        r.ag[slot, 0:MAIN, mine] = rows[:MAIN].astype(BF)
        r.rows_ext[...] = rows[M:]
        for b in range(EX):
            r.send_ext[i, b] = r.rows_ext[b * EXT : (b + 1) * EXT, :].astype(BF)
        r.recv_ext[i, 0] = r.rows_ext[0:EXT, :].astype(BF)

    rows_for(0, 0)
    pl.semaphore_wait(barrier, EX - 1 + NT - 1)
    for b in range(1, EX):
        nb = opposite(b)
        remote(
            r.send_main.at[0, pl.ds(b * MAIN, MAIN), :], r.ag.at[0, pl.ds(nb * MAIN, MAIN), mine],
            r.out_sem.at[0], r.a2a_sem.at[nb // (EX // 2)], peer(b),
        ).start()
        remote(
            r.send_ext.at[0, b], r.recv_ext.at[0, nb], r.out_sem.at[1], r.a2a_sem.at[2], peer(b)
        ).start()

    for name in ("tok_a", "gain_a", "vw", "gw"):
        loads[name].wait()
    squares = jnp.zeros((T, F), F32)
    for j in range(NT):
        v = r.v_tok_a[:, j * F : (j + 1) * F].astype(F32)
        squares = squares + v * v
    inv_a = lax.rsqrt(jnp.sum(squares, axis=1, keepdims=True) / D + 1e-6)
    for j in range(NT):
        cols = slice(j * F, (j + 1) * F)
        v = r.v_tok_a[:, cols].astype(F32) * inv_a * r.v_gain_a[j : j + 1, :]
        r.normed_a[:, cols] = v.astype(BF)
    value = dot(r.normed_a[...], r.v_vw[...])
    gate = dot(r.normed_a[...], r.v_gw[...])
    glu = (value / (1.0 + jnp.exp(-gate))).astype(BF)
    r.padded[32:, :] = glu.astype(F32)
    r.tail[...] = glu[T - 32 :, :]
    halo = remote(r.tail, r.halo, r.out_sem.at[4], r.halo_sem, (lax.rem(e + 1, EX), t))
    halo.start()

    weight = r.weight[...]
    w_hi = weight.astype(BF)
    w_lo = (weight - w_hi.astype(F32)).astype(BF)
    r.w_hi[...] = (r.picks[...].astype(F32) * dot(r.spread[0:EX, :], w_hi, 0, 0)).astype(BF)
    r.w_lo[...] = (r.picks[...].astype(F32) * dot(r.spread[0:EX, :], w_lo, 0, 0)).astype(BF)

    cuts = [(EX * i // 4) * MAIN for i in range(4)] + [S]
    pieces = [pl.ds(a, b - a) for a, b in zip(cuts, cuts[1:])]

    def pass_on(sign, k, piece):
        return remote(
            r.ag.at[turn(-sign * (k - 1) * way), pieces[piece], mine],
            r.ag.at[turn(-sign * k * way), pieces[piece], mine],
            r.out_sem.at[8], r.ag_in.at[k - 1 if sign > 0 else LA + k - 1, piece], tp_of(sign * way),
        )

    def to_mate(slot):
        return remote(
            r.ag.at[slot, :, mine], r.ag.at[slot, :, mine], r.out_sem.at[9], r.am_in.at[slot], mate
        )

    def bulk(ref, sem):
        return pltpu.make_async_copy(ref, ref, sem)

    def settle_ext(i, slot):
        for b in range(EX):
            r.rows_ext[b * EXT : (b + 1) * EXT, :] = r.recv_ext[i, b].astype(F32)
        r.ag[slot, M:S, mine] = r.rows_ext[...].astype(BF)

    def convolve():
        loads["ker"].wait()
        halo.wait_recv()
        r.padded[0:32, :] = jnp.where(e > 0, r.halo[...].astype(F32), 0.0)
        mixed = jnp.zeros((T, F), F32)
        for tap in range(g.TAPS):
            low = 32 - (g.TAPS - 1) + tap
            mixed = mixed + r.v_ker[tap : tap + 1, :] * r.padded[low : low + T, :]
        r.mixed[...] = mixed
        ones = jnp.ones((8, F), F32)
        sums = dot(ones, mixed, 1, 1, lax.Precision.HIGHEST)
        powers = dot(ones, mixed * mixed, 1, 1, lax.Precision.HIGHEST)
        r.stats[0] = jnp.where(iota((8, T), 0) == 0, sums, powers)[0:2]

        for i in range(1, NT):
            remote(
                r.stats.at[0], r.stats.at[NT - i], r.out_sem.at[5], r.stat_sem, tps[i]
            ).start()

    bulk(r.ag.at[0, pl.ds(MAIN, HALF - MAIN), mine], r.a2a_sem.at[0]).wait()
    for piece in (0, 1):
        if LA:
            pass_on(1, 1, piece).start()
        if LB:
            pass_on(-1, 1, piece).start()
    for i in range(DN):
        rows_for(1 + i, near + i)
    for b in range(1, EX if DN else 0):
        nb = opposite(b)
        remote(
            r.send_main.at[pl.ds(1, DN), pl.ds(b * MAIN, MAIN), :],
            r.ag.at[pl.ds(near, DN), pl.ds(nb * MAIN, MAIN), mine],
            r.out_sem.at[2], r.a2a_sem.at[3], peer(b),
        ).start()
        remote(
            r.send_ext.at[pl.ds(1, DN), b], r.recv_ext.at[pl.ds(1, DN), nb],
            r.out_sem.at[3], r.a2a_sem.at[4], peer(b),
        ).start()
    convolve()
    bulk(r.ag.at[0, pl.ds(HALF, HALF), mine], r.a2a_sem.at[1]).wait()
    bulk(r.recv_ext.at[0, pl.ds(1, EX - 1)], r.a2a_sem.at[2]).wait()
    settle_ext(0, 0)
    for piece in (2, 3):
        if LA:
            pass_on(1, 1, piece).start()
        if LB:
            pass_on(-1, 1, piece).start()
    to_mate(0).start()

    def c_mate(slot):
        return remote(
            r.c_part.at[turn(y + slot) * 2 + 1 - core], r.c_pair.at[slot],
            r.out_sem.at[10], r.cm_in, mate,
        )

    def channel_norm():
        loads["cg"].wait()
        loads["ow"].wait()
        bulk(r.stats.at[pl.ds(1, NT - 1)], r.stat_sem).wait()
        total = r.stats[0]
        for j in range(1, NT):
            total = total + r.stats[j]
        average = total[0:1] / g.CH
        scale = lax.rsqrt(total[1:2] / g.CH - average * average + 1e-5)
        line = iota((8, T), 0)
        both = jnp.where(line == 0, average, jnp.where(line == 1, scale, 0.0))
        line = iota((8, F), 0)
        high = lax.Precision.HIGHEST
        average = dot(both, jnp.where(line == 0, 1.0, 0.0), 0, 0, high)
        scale = dot(both, jnp.where(line == 1, 1.0, 0.0), 0, 0, high)
        act = silu((r.mixed[...] - average) * scale * r.v_cg[...]).astype(BF)
        for j in range(NT):
            r.c_part[j] = dot(act, r.v_ow[:, j * F : (j + 1) * F]).astype(BF)
        for slot in range(Y):
            c_mate(slot).start()

    def c_sum(slot):
        mine_part = r.c_part[turn(y + slot) * 2 + core].astype(F32)
        return mine_part + r.c_pair[slot].astype(F32)

    def hop(k, sign):
        return H - k if sign > 0 else 2 * H - 1 - k

    def c_link(k, sign):
        n = hop(k, sign)
        return remote(
            r.c_stage.at[n], r.c_got.at[n], r.out_sem.at[11], r.c_in.at[n], tp_of(sign * way)
        )

    def c_step(k, sign):
        part = c_sum(turn(sign * k * way))
        if k < (H if sign > 0 else H - 1):
            c_link(k + 1, sign).wait_recv()
            part = part + r.c_got[hop(k + 1, sign)].astype(F32)
        r.c_stage[hop(k, sign)] = part.astype(BF)
        c_link(k, sign).start()

    def c_both(k):
        if k == H:
            bulk(r.c_pair, r.cm_in).wait()
        c_step(k, 1)
        if k < H:
            c_step(k, -1)

    TILE = S // g.TILES

    def experts_in(slot, first):
        to_mate(slot).wait_recv()
        cols = pl.ds(pl.multiple_of(turn(y + slot) * 2 * F, 2 * F), 2 * F)
        wg, wu = r.v_eg[:, cols], r.v_eu[:, cols]
        for i in range(g.TILES):
            part = pl.ds(i * TILE, TILE)
            lhs = r.ag[slot, part, :]
            a, b = dot(lhs, wg, 1, 1), dot(lhs, wu, 1, 1)
            r.gate[part, :] = a if first else r.gate[part, :] + a
            r.up[part, :] = b if first else r.up[part, :] + b

    loads["eg"].wait()
    loads["eu"].wait()
    steps = list(range(H, 0, -1))
    waiting = [0]

    def take_direct():
        bulk(r.ag.at[pl.ds(near, DN), pl.ds(MAIN, M - MAIN), mine], r.a2a_sem.at[3]).wait()
        bulk(r.recv_ext.at[pl.ds(1, DN), pl.ds(1, EX - 1)], r.a2a_sem.at[4]).wait()
        for i in range(DN):
            settle_ext(1 + i, near + i)
            to_mate(near + i).start()
        return [H] if DN == 2 else [near + i for i in range(DN)]

    for k in range(1, LA + 1):
        if DN and k == g.DIRECT_AT:
            waiting = waiting + take_direct()
        down, up = turn(-k * way), turn(k * way)
        for piece in range(4):
            pass_on(1, k, piece).wait_recv()
            if k < LA:
                pass_on(1, k + 1, piece).start()
            if k <= LB:
                pass_on(-1, k, piece).wait_recv()
                if k < LB:
                    pass_on(-1, k + 1, piece).start()
        to_mate(down).start()
        if k <= LB:
            to_mate(up).start()
        for i, slot in enumerate(waiting):
            experts_in(slot, k == 1 and i == 0)
        waiting = [up, down] if k <= LB else [down]
        if k == 1:
            channel_norm()
        elif k == 2:
            c_both(steps.pop(0))
    c_both(steps.pop(0))
    if DN == 2:
        waiting = waiting + [turn((H - 1) * way)]
    for slot in waiting[:-1]:
        experts_in(slot, False)
    loads["ed"].wait()
    if len(steps) > 2:
        c_both(steps.pop(0))

    def m_mate(slot, piece):
        part = slice(None) if piece is None else pieces[piece]
        return remote(
            r.m_full.at[slot, part, other], r.m_pair.at[slot, part, :],
            r.out_sem.at[12], r.mm_in.at[slot if piece is None else Y + piece], mate,
        )

    def produce(slot):
        cols = pl.ds(pl.multiple_of(turn(y + slot) * 2 * F, 2 * F), 2 * F)
        r.m_full[slot] = dot(r.hidden[...], r.v_ed[:, cols]).astype(BF)
        m_mate(slot, None).start()

    def m_link(k, sign, piece):
        n, part = hop(k, sign), pieces[piece]
        return remote(
            r.m_stage.at[n, part, :], r.m_got.at[n, part, :],
            r.out_sem.at[13], r.m_in.at[n, piece], tp_of(sign * way),
        )

    def pair_sum(slot, piece):
        part = pieces[piece]
        return r.m_full[slot, part, mine].astype(F32) + r.m_pair[slot, part, :].astype(F32)

    def m_step(k, sign, piece):
        part = pieces[piece]
        total = pair_sum(turn(sign * k * way), piece)
        if k < (H if sign > 0 else H - 1):
            m_link(k + 1, sign, piece).wait_recv()
            total = total + r.m_got[hop(k + 1, sign), part, :].astype(F32)
        r.m_stage[hop(k, sign), part, :] = total.astype(BF)
        m_link(k, sign, piece).start()

    to_mate(waiting[-1]).wait_recv()
    far = H

    def wide(slot):
        return pl.ds(pl.multiple_of(turn(y + slot) * 2 * F, 2 * F), 2 * F)

    cols = wide(waiting[-1])
    wg, wu = r.v_eg[:, cols], r.v_eu[:, cols]
    for piece in (3, 2, 1, 0):
        part = pieces[piece]
        lhs = r.ag[waiting[-1], part, :]
        a = r.gate[part, :] + dot(lhs, wg, 1, 1)
        b = r.up[part, :] + dot(lhs, wu, 1, 1)
        hidden = (silu(a) * b).astype(BF)
        r.hidden[part, :] = hidden
        r.m_full[far, part, :] = dot(hidden, r.v_ed[:, wide(far)]).astype(BF)
        m_mate(far, piece).start()
    for piece in (3, 2, 1, 0):
        m_mate(far, piece).wait_recv()
        m_step(H, 1, piece)
        if piece == 3:
            produce(turn(-(H - 1) * way))
    produce(turn((H - 1) * way))
    if H > 1:
        m_mate(turn(-(H - 1) * way), None).wait_recv()
        for piece in (3, 2, 1, 0):
            m_step(H - 1, -1, piece)
    if H > 2:
        for slot in (turn(-(H - 2) * way), turn((H - 2) * way)):
            produce(slot)
    for k in range(H - 1, 0, -1):
        m_mate(turn(k * way), None).wait_recv()
        for piece in (3, 2, 1, 0):
            m_step(k, 1, piece)
            if k > 1:
                if piece == 3:
                    m_mate(turn(-(k - 1) * way), None).wait_recv()
                m_step(k - 1, -1, piece)
        if k > 2:
            for slot in (turn(-(k - 2) * way), turn((k - 2) * way)):
                produce(slot)
        elif k == 2 or H == 2:
            produce(0)
        if k == g.C_AT and len(steps) > 1:
            c_both(steps.pop(0))

    m_mate(0, None).wait_recv()
    for piece in (3, 2, 1, 0):
        part = pieces[piece]
        total = pair_sum(0, piece)
        for sign in (1, -1):
            m_link(1, sign, piece).wait_recv()
            total = total + r.m_got[hop(1, sign), part, :].astype(F32)
        r.back[part, :] = total.astype(BF)
        if piece == 3:
            r.rows_ext[...] = total[M - cuts[3] :]
            for b in range(EX):
                r.back_ext[b] = r.rows_ext[b * EXT : (b + 1) * EXT, :].astype(BF)
        for b in range(EX * (piece + 1) // 4 - 1, max(EX * piece // 4, 1) - 1, -1):
            remote(
                r.back.at[pl.ds(b * MAIN, MAIN), :], r.home.at[pl.ds(opposite(b) * MAIN, MAIN), :],
                r.out_sem.at[6], r.home_sem.at[0], peer(b),
            ).start()
        if piece == 3:
            for b in range(EX - 1, 0, -1):
                remote(
                    r.back_ext.at[b], r.home_ext.at[opposite(b)],
                    r.out_sem.at[7], r.home_sem.at[1], peer(b),
                ).start()
    r.home[0:MAIN, :] = r.back[0:MAIN, :]
    r.home_ext[0] = r.back_ext[0]

    while steps:
        c_both(steps.pop(0))
    total = c_sum(0)
    for sign in (1, -1):
        c_link(1, sign).wait_recv()
        total = total + r.c_got[hop(1, sign)].astype(F32)
    r.conv_out[...] = jnp.transpose(total).astype(BF)

    bulk(r.home_ext.at[pl.ds(1, EX - 1)], r.home_sem.at[1]).wait()
    for b in range(EX):
        r.rows_ext[b * EXT : (b + 1) * EXT, :] = r.home_ext[b].astype(F32)
    r.home[M:S, :] = r.rows_ext[...].astype(BF)
    bulk(r.home.at[pl.ds(MAIN, M - MAIN), :], r.home_sem.at[0]).wait()
    result = dot(r.w_hi[...], r.home[...], 0, 0) + dot(r.w_lo[...], r.home[...], 0, 0)
    r.moe_out[...] = result.astype(BF)

    bulk(r.send_main.at[0, pl.ds(MAIN, M - MAIN), :], r.out_sem.at[0]).wait()
    bulk(r.send_ext.at[0, pl.ds(1, EX - 1)], r.out_sem.at[1]).wait()
    if DN:
        bulk(r.send_main.at[pl.ds(1, DN), pl.ds(MAIN, M - MAIN), :], r.out_sem.at[2]).wait()
        bulk(r.send_ext.at[pl.ds(1, DN), pl.ds(1, EX - 1)], r.out_sem.at[3]).wait()
    halo.wait_send()
    bulk(r.stats.at[pl.ds(1, NT - 1)], r.out_sem.at[5]).wait()
    bulk(r.back.at[pl.ds(MAIN, M - MAIN), :], r.out_sem.at[6]).wait()
    bulk(r.back_ext.at[pl.ds(1, EX - 1)], r.out_sem.at[7]).wait()
    if LA + LB:
        bulk(r.ag.at[pl.ds(0, LA + LB), :, mine], r.out_sem.at[8]).wait()
    bulk(r.ag.at[:, :, mine], r.out_sem.at[9]).wait()
    bulk(r.c_part.at[pl.ds(0, Y)], r.out_sem.at[10]).wait()
    bulk(r.c_stage, r.out_sem.at[11]).wait()
    bulk(r.m_full.at[:, :, other], r.out_sem.at[12]).wait()
    bulk(r.m_stage, r.out_sem.at[13]).wait()


def run(Z, X, args):
    (tok_a, gain_a, vw, gw, ker, cg, ow, tok_b, gain_b, routes, logits, eg, eu, ed) = args
    EX, NT = lax.axis_size("ep"), lax.axis_size("tp")
    T, D = tok_a.shape
    R, F, HU = tok_b.shape[0], vw.shape[1], eg.shape[2]
    cap = 3 * R * routes.shape[1] // (2 * EX)
    EXT, Y, DN = cap - MAIN, NT // 2, 2
    S, M = EX * cap, EX * MAIN
    given = dict(
        tok_b=tok_b, routes=routes.T, logits=logits.T, gain_b=gain_b.reshape(NT, F),
        tok_a=tok_a, gain_a=gain_a.reshape(NT, F), vw=vw, gw=gw, ker=ker, cg=cg.reshape(1, F),
        ow=ow, eg=eg[0].T, eu=eu[0].T, ed=ed[0],
    )
    vm, dma = pltpu.VMEM, pltpu.SemaphoreType.DMA
    scratch = dict(
        {"v_" + n: vm(given[n].shape, given[n].dtype) for n in INPUTS},
        in_sem=dma((len(INPUTS),)), spread=vm((EX + 8, S), BF), code=vm((EX + 8, R), F32),
        picks=vm((S, R), BF), weight=vm((EX, R), F32), w_hi=vm((S, R), BF), w_lo=vm((S, R), BF),
        send_main=vm((DN + 1, M, F), BF), send_ext=vm((DN + 1, EX, EXT, F), BF),
        recv_ext=vm((DN + 1, EX, EXT, F), BF),
        rows_ext=vm((EX * EXT, F), F32), ag=vm((Y, S, 2 * F), BF),
        out_sem=dma((14,)), a2a_sem=dma((5,)), normed_a=vm((T, D), BF), padded=vm((T + 32, F), F32),
        tail=vm((32, F), BF), halo=vm((32, F), BF), halo_sem=dma, mixed=vm((T, F), F32),
        stats=vm((NT, 2, T), F32), stat_sem=dma,
        ag_in=dma((max(Y - 1 - DN, 1), 4)), am_in=dma((Y,)),
        c_part=vm((NT, T, F), BF), c_pair=vm((Y, T, F), BF), c_stage=vm((Y - 1, T, F), BF),
        c_got=vm((Y - 1, T, F), BF), cm_in=dma, c_in=dma((Y - 1,)),
        gate=vm((S, HU), F32), up=vm((S, HU), F32), hidden=vm((S, HU), BF),
        m_full=vm((Y, S, 2 * F), BF), m_pair=vm((Y, S, F), BF), m_stage=vm((Y - 1, S, F), BF),
        m_got=vm((Y - 1, S, F), BF), mm_in=dma((Y + 4,)), m_in=dma((Y - 1, 4)), back=vm((S, F), BF), back_ext=vm((EX, EXT, F), BF),
        home=vm((S, F), BF), home_ext=vm((EX, EXT, F), BF), home_sem=dma((2,)),
    )
    names = ["in_" + n for n in INPUTS] + ["conv_out", "moe_out"] + list(scratch)
    g = SimpleNamespace(
        names=names, Z=Z, X=X, Y=Y, F=F, EX=EX, EXT=EXT, NT=NT, T=T, R=R, D=D, S=S, CH=NT * F,
        TAPS=ker.shape[0], TILES=3, DN=DN, DIRECT_AT=max(NT // 4 - (DN + 1) // 2, 1), C_AT=2,
    )
    conv_out, moe_out = pl.pallas_call(
        functools.partial(kernel, g),
        out_shape=(pltpu.VMEM((F, T), BF), pltpu.VMEM((R, F), BF)),
        in_specs=[pl.BlockSpec(memory_space=pl.ANY)] * len(INPUTS),
        out_specs=(pl.BlockSpec(memory_space=pltpu.VMEM),) * 2,
        scratch_shapes=list(scratch.values()),
        compiler_params=pltpu.CompilerParams(
            collective_id=0, has_side_effects=True, vmem_limit_bytes=60 * 1024 * 1024
        ),
    )(*[given[n] for n in INPUTS])
    return conv_out, moe_out.T


def solution(mesh, Z=8, X=4):
    return jax.shard_map(
        lambda *args: run(Z, X, args),
        mesh=mesh,
        in_specs=(
            P("ep", None), P(), P(None, "tp"), P(None, "tp"), P(None, "tp"), P("tp"), P("tp", None),
            P("ep", None), P(), P("ep", None), P("ep", None), P("ep", None, "tp"),
            P("ep", None, "tp"), P("ep", "tp", None),
        ),
        out_specs=(P("tp", "ep"), P("tp", "ep")),
        check_vma=False,
    )
```

```python
import functools
from types import SimpleNamespace

import jax
import jax.numpy as jnp
from jax import lax
from jax.experimental import pallas as pl
from jax.experimental.pallas import tpu as pltpu
from jax.sharding import PartitionSpec as P

MESH = pl.DeviceIdType.MESH
BF = jnp.bfloat16
F32 = jnp.float32
I32 = jnp.int32
MAIN = 16
INPUTS = (
    "routes", "logits", "tok_b", "gain_b", "tok_a", "gain_a", "vw", "gw",
    "ker", "cg", "ow", "eg", "eu", "ed",
)


def iota(shape, dim):
    return lax.broadcasted_iota(I32, shape, dim)


def dot(a, b, ca=1, cb=0, precision=None):
    return lax.dot_general(
        a, b, (((ca,), (cb,)), ((), ())), precision=precision, preferred_element_type=F32
    )


def silu(v):
    return v / (1.0 + jnp.exp(-v))


def kernel(g, *refs):
    r = SimpleNamespace(**dict(zip(g.names, refs)))
    Z, X, Y, F, EX, EXT = g.Z, g.X, g.Y, g.F, g.EX, g.EXT
    NT, T, R, D, S = g.NT, g.T, g.R, g.D, g.S
    M = EX * MAIN
    HALF = M // 2
    H, DN = Y // 2, g.DN
    LA, LB = H - (DN + 1) // 2, H - 1 - DN // 2
    e = lax.axis_index("ep")
    t = lax.axis_index("tp")
    core, y = lax.rem(t, 2), lax.div(t, 2)
    z, x = lax.div(e, X), lax.rem(e, X)
    way = 1 - 2 * core
    mate = (e, t + way)
    mine = pl.ds(pl.multiple_of(core * F, F), F)
    other = pl.ds(pl.multiple_of((1 - core) * F, F), F)
    near = H - 1 + core if DN == 2 else H - DN // 2

    def turn(a):
        return lax.rem(a + 4 * Y, Y)

    def tp_of(step):
        return (e, turn(y + step) * 2 + core)

    def place(b):
        i, dx = b // X, b % X
        dz = jnp.where(i % 2 == 1, (i + 1) // 2, Z - i // 2)
        return lax.rem(z + dz, Z) * X + lax.rem(x + dx, X)

    rows_of = [lax.rem(z + i, Z) * X for i in range(Z)]
    cols_of = [lax.rem(x + i, X) for i in range(X)]

    def peer(b):
        i, dx = divmod(b, X)
        dz = ((i + 1) // 2 if i % 2 else Z - i // 2) % Z
        return (rows_of[dz] + cols_of[dx], t)

    def opposite(b):
        i, dx = divmod(b, X)
        back = i if i in (0, Z - 1) else (i + 1 if i % 2 else i - 1)
        return back * X + (X - dx) % X

    def remote(src, dst, send, recv, to):
        return pltpu.make_async_remote_copy(
            src_ref=src, dst_ref=dst, send_sem=send, recv_sem=recv, device_id=to, device_id_type=MESH
        )

    loads = {}
    for i, name in enumerate(INPUTS):
        loads[name] = pltpu.make_async_copy(
            getattr(r, "in_" + name), getattr(r, "v_" + name), r.in_sem.at[i]
        )
    for name in INPUTS[:4]:
        loads[name].start()

    barrier = pltpu.get_barrier_semaphore()

    for b in range(EX - 1, 0, -1):
        pl.semaphore_signal(barrier, 1, device_id=peer(b), device_id_type=MESH)
    tps = [(e, lax.rem(t + i, NT)) for i in range(NT)]
    for i in range(1, NT):
        pl.semaphore_signal(barrier, 1, device_id=tps[i], device_id_type=MESH)
    for name in INPUTS[4:]:
        loads[name].start()

    s = iota((1, S), 1)
    block = jnp.where(s < M, s // MAIN, (s - M) // EXT)
    rank = jnp.where(s < M, s % MAIN, MAIN + (s - M) % EXT) + 1
    line = iota((EX + 8, S), 0)
    spread = jnp.where(line == place(block), 1.0, jnp.where(line == EX, rank.astype(F32), 0.0))
    r.spread[...] = spread.astype(BF)
    for name in ("routes", "logits"):
        loads[name].wait()
    lines = iota((EX, R), 0)
    first = jnp.where(lines == r.v_routes[0:1, :], 1.0, 0.0)
    second = jnp.where(lines == r.v_routes[1:2, :], 1.0, 0.0)
    named = first + second
    earlier = jnp.where(iota((R, R), 0) < iota((R, R), 1), 1.0, 0.0).astype(BF)
    r.code[0:EX, :] = named * (dot(named.astype(BF), earlier) + 1.0)
    r.code[EX:, :] = jnp.where(iota((8, R), 0) == 0, -1.0, 0.0)
    l0, l1 = r.v_logits[0:1, :], r.v_logits[1:2, :]
    top = jnp.maximum(l0, l1)
    e0, e1 = jnp.exp(l0 - top), jnp.exp(l1 - top)
    weight = first * (e0 / (e0 + e1)) + second * (e1 / (e0 + e1))
    r.weight[...] = weight

    for name in ("tok_b", "gain_b"):
        loads[name].wait()
    squares = jnp.zeros((R, F), F32)
    for j in range(NT):
        v = r.v_tok_b[:, j * F : (j + 1) * F].astype(F32)
        squares = squares + v * v
    inv = lax.rsqrt(jnp.sum(squares, axis=1, keepdims=True) / D + 1e-6)

    lag = dot(r.spread[...], r.code[...].astype(BF), 0, 0)
    r.picks[...] = jnp.where(lag == 0.0, 1.0, 0.0).astype(BF)

    def rows_for(i, slot):
        col = turn(y + slot) * 2 + core
        own = r.v_tok_b[:, pl.ds(pl.multiple_of(col * F, F), F)].astype(F32)
        normed = (own * inv * r.v_gain_b[pl.ds(col, 1), :]).astype(BF)
        rows = dot(r.picks[...], normed)
        r.send_main[i] = rows[:M].astype(BF)
        r.ag[slot, 0:MAIN, mine] = rows[:MAIN].astype(BF)
        r.rows_ext[...] = rows[M:]
        for b in range(EX):
            r.send_ext[i, b] = r.rows_ext[b * EXT : (b + 1) * EXT, :].astype(BF)
        r.recv_ext[i, 0] = r.rows_ext[0:EXT, :].astype(BF)

    rows_for(0, 0)
    pl.semaphore_wait(barrier, EX - 1 + NT - 1)
    for b in range(1, EX):
        nb = opposite(b)
        remote(
            r.send_main.at[0, pl.ds(b * MAIN, MAIN), :], r.ag.at[0, pl.ds(nb * MAIN, MAIN), mine],
            r.out_sem.at[0], r.a2a_sem.at[nb // (EX // 2)], peer(b),
        ).start()
        remote(
            r.send_ext.at[0, b], r.recv_ext.at[0, nb], r.out_sem.at[1], r.a2a_sem.at[2], peer(b)
        ).start()

    for name in ("tok_a", "gain_a", "vw", "gw"):
        loads[name].wait()
    squares = jnp.zeros((T, F), F32)
    for j in range(NT):
        v = r.v_tok_a[:, j * F : (j + 1) * F].astype(F32)
        squares = squares + v * v
    inv_a = lax.rsqrt(jnp.sum(squares, axis=1, keepdims=True) / D + 1e-6)
    for j in range(NT):
        cols = slice(j * F, (j + 1) * F)
        v = r.v_tok_a[:, cols].astype(F32) * inv_a * r.v_gain_a[j : j + 1, :]
        r.normed_a[:, cols] = v.astype(BF)
    value = dot(r.normed_a[...], r.v_vw[...])
    gate = dot(r.normed_a[...], r.v_gw[...])
    glu = (value / (1.0 + jnp.exp(-gate))).astype(BF)
    r.padded[32:, :] = glu.astype(F32)
    r.tail[...] = glu[T - 32 :, :]
    halo = remote(r.tail, r.halo, r.out_sem.at[4], r.halo_sem, (lax.rem(e + 1, EX), t))
    halo.start()

    weight = r.weight[...]
    w_hi = weight.astype(BF)
    w_lo = (weight - w_hi.astype(F32)).astype(BF)
    r.w_hi[...] = (r.picks[...].astype(F32) * dot(r.spread[0:EX, :], w_hi, 0, 0)).astype(BF)
    r.w_lo[...] = (r.picks[...].astype(F32) * dot(r.spread[0:EX, :], w_lo, 0, 0)).astype(BF)

    cuts = [(EX * i // 4) * MAIN for i in range(4)] + [S]
    pieces = [pl.ds(a, b - a) for a, b in zip(cuts, cuts[1:])]

    def pass_on(sign, k, piece):
        return remote(
            r.ag.at[turn(-sign * (k - 1) * way), pieces[piece], mine],
            r.ag.at[turn(-sign * k * way), pieces[piece], mine],
            r.out_sem.at[8], r.ag_in.at[k - 1 if sign > 0 else LA + k - 1, piece], tp_of(sign * way),
        )

    def to_mate(slot):
        return remote(
            r.ag.at[slot, :, mine], r.ag.at[slot, :, mine], r.out_sem.at[9], r.am_in.at[slot], mate
        )

    def bulk(ref, sem):
        return pltpu.make_async_copy(ref, ref, sem)

    def settle_ext(i, slot):
        for b in range(EX):
            r.rows_ext[b * EXT : (b + 1) * EXT, :] = r.recv_ext[i, b].astype(F32)
        r.ag[slot, M:S, mine] = r.rows_ext[...].astype(BF)

    def convolve():
        loads["ker"].wait()
        halo.wait_recv()
        r.padded[0:32, :] = jnp.where(e > 0, r.halo[...].astype(F32), 0.0)
        mixed = jnp.zeros((T, F), F32)
        for tap in range(g.TAPS):
            low = 32 - (g.TAPS - 1) + tap
            mixed = mixed + r.v_ker[tap : tap + 1, :] * r.padded[low : low + T, :]
        r.mixed[...] = mixed
        ones = jnp.ones((8, F), F32)
        sums = dot(ones, mixed, 1, 1, lax.Precision.HIGHEST)
        powers = dot(ones, mixed * mixed, 1, 1, lax.Precision.HIGHEST)
        r.stats[0] = jnp.where(iota((8, T), 0) == 0, sums, powers)[0:2]

        for i in range(1, NT):
            remote(
                r.stats.at[0], r.stats.at[NT - i], r.out_sem.at[5], r.stat_sem, tps[i]
            ).start()

    bulk(r.ag.at[0, pl.ds(MAIN, HALF - MAIN), mine], r.a2a_sem.at[0]).wait()
    for piece in (0, 1):
        if LA:
            pass_on(1, 1, piece).start()
        if LB:
            pass_on(-1, 1, piece).start()
    for i in range(DN):
        rows_for(1 + i, near + i)
    for b in range(1, EX if DN else 0):
        nb = opposite(b)
        remote(
            r.send_main.at[pl.ds(1, DN), pl.ds(b * MAIN, MAIN), :],
            r.ag.at[pl.ds(near, DN), pl.ds(nb * MAIN, MAIN), mine],
            r.out_sem.at[2], r.a2a_sem.at[3], peer(b),
        ).start()
        remote(
            r.send_ext.at[pl.ds(1, DN), b], r.recv_ext.at[pl.ds(1, DN), nb],
            r.out_sem.at[3], r.a2a_sem.at[4], peer(b),
        ).start()
    convolve()
    bulk(r.ag.at[0, pl.ds(HALF, HALF), mine], r.a2a_sem.at[1]).wait()
    bulk(r.recv_ext.at[0, pl.ds(1, EX - 1)], r.a2a_sem.at[2]).wait()
    settle_ext(0, 0)
    for piece in (2, 3):
        if LA:
            pass_on(1, 1, piece).start()
        if LB:
            pass_on(-1, 1, piece).start()
    to_mate(0).start()

    def c_mate(slot):
        return remote(
            r.c_part.at[turn(y + slot) * 2 + 1 - core], r.c_pair.at[slot],
            r.out_sem.at[10], r.cm_in, mate,
        )

    def channel_norm():
        loads["cg"].wait()
        loads["ow"].wait()
        bulk(r.stats.at[pl.ds(1, NT - 1)], r.stat_sem).wait()
        total = r.stats[0]
        for j in range(1, NT):
            total = total + r.stats[j]
        average = total[0:1] / g.CH
        scale = lax.rsqrt(total[1:2] / g.CH - average * average + 1e-5)
        line = iota((8, T), 0)
        both = jnp.where(line == 0, average, jnp.where(line == 1, scale, 0.0))
        line = iota((8, F), 0)
        high = lax.Precision.HIGHEST
        average = dot(both, jnp.where(line == 0, 1.0, 0.0), 0, 0, high)
        scale = dot(both, jnp.where(line == 1, 1.0, 0.0), 0, 0, high)
        act = silu((r.mixed[...] - average) * scale * r.v_cg[...]).astype(BF)
        for j in range(NT):
            r.c_part[j] = dot(act, r.v_ow[:, j * F : (j + 1) * F]).astype(BF)
        for slot in range(Y):
            c_mate(slot).start()

    def c_sum(slot):
        mine_part = r.c_part[turn(y + slot) * 2 + core].astype(F32)
        return mine_part + r.c_pair[slot].astype(F32)

    def hop(k, sign):
        return H - k if sign > 0 else 2 * H - 1 - k

    def c_link(k, sign):
        n = hop(k, sign)
        return remote(
            r.c_stage.at[n], r.c_got.at[n], r.out_sem.at[11], r.c_in.at[n], tp_of(sign * way)
        )

    def c_step(k, sign):
        part = c_sum(turn(sign * k * way))
        if k < (H if sign > 0 else H - 1):
            c_link(k + 1, sign).wait_recv()
            part = part + r.c_got[hop(k + 1, sign)].astype(F32)
        r.c_stage[hop(k, sign)] = part.astype(BF)
        c_link(k, sign).start()

    def c_both(k):
        if k == H:
            bulk(r.c_pair, r.cm_in).wait()
        c_step(k, 1)
        if k < H:
            c_step(k, -1)

    TILE = S // g.TILES

    def experts_in(slot, first):
        to_mate(slot).wait_recv()
        cols = pl.ds(pl.multiple_of(turn(y + slot) * 2 * F, 2 * F), 2 * F)
        wg, wu = r.v_eg[:, cols], r.v_eu[:, cols]
        for i in range(g.TILES):
            part = pl.ds(i * TILE, TILE)
            lhs = r.ag[slot, part, :]
            a, b = dot(lhs, wg, 1, 1), dot(lhs, wu, 1, 1)
            r.gate[part, :] = a if first else r.gate[part, :] + a
            r.up[part, :] = b if first else r.up[part, :] + b

    loads["eg"].wait()
    loads["eu"].wait()
    steps = list(range(H, 0, -1))
    waiting = [0]

    def take_direct():
        bulk(r.ag.at[pl.ds(near, DN), pl.ds(MAIN, M - MAIN), mine], r.a2a_sem.at[3]).wait()
        bulk(r.recv_ext.at[pl.ds(1, DN), pl.ds(1, EX - 1)], r.a2a_sem.at[4]).wait()
        for i in range(DN):
            settle_ext(1 + i, near + i)
            to_mate(near + i).start()
        return [H] if DN == 2 else [near + i for i in range(DN)]

    for k in range(1, LA + 1):
        if DN and k == g.DIRECT_AT:
            if k > 1:
                early, waiting = waiting, take_direct()
            else:
                waiting = waiting + take_direct()
        down, up = turn(-k * way), turn(k * way)
        for piece in range(4):
            if k == LA and k > 1 and piece == 2:
                for slot in early:
                    experts_in(slot, False)
            pass_on(1, k, piece).wait_recv()
            if k < LA:
                pass_on(1, k + 1, piece).start()
            if k <= LB:
                pass_on(-1, k, piece).wait_recv()
                if k < LB:
                    pass_on(-1, k + 1, piece).start()
        to_mate(down).start()
        if k <= LB:
            to_mate(up).start()
        for i, slot in enumerate(waiting):
            experts_in(slot, k == 1 and i == 0)
        waiting = [up, down] if k <= LB else [down]
        if k == 1:
            channel_norm()
        elif k == 2:
            c_both(steps.pop(0))
    c_both(steps.pop(0))
    if DN == 2:
        waiting = waiting + [turn((H - 1) * way)]
    for slot in waiting[:-1]:
        experts_in(slot, False)
    loads["ed"].wait()
    if len(steps) > 2:
        c_both(steps.pop(0))

    def m_mate(slot, piece):
        part = slice(None) if piece is None else pieces[piece]
        return remote(
            r.m_full.at[slot, part, other], r.m_pair.at[slot, part, :],
            r.out_sem.at[12], r.mm_in.at[slot if piece is None else Y + piece], mate,
        )

    def produce(slot):
        cols = pl.ds(pl.multiple_of(turn(y + slot) * 2 * F, 2 * F), 2 * F)
        r.m_full[slot] = dot(r.hidden[...], r.v_ed[:, cols]).astype(BF)
        m_mate(slot, None).start()

    def m_link(k, sign, piece):
        n, part = hop(k, sign), pieces[piece]
        return remote(
            r.m_stage.at[n, part, :], r.m_got.at[n, part, :],
            r.out_sem.at[13], r.m_in.at[n, piece], tp_of(sign * way),
        )

    def pair_sum(slot, piece):
        part = pieces[piece]
        return r.m_full[slot, part, mine].astype(F32) + r.m_pair[slot, part, :].astype(F32)

    def m_step(k, sign, piece):
        part = pieces[piece]
        total = pair_sum(turn(sign * k * way), piece)
        if k < (H if sign > 0 else H - 1):
            m_link(k + 1, sign, piece).wait_recv()
            total = total + r.m_got[hop(k + 1, sign), part, :].astype(F32)
        r.m_stage[hop(k, sign), part, :] = total.astype(BF)
        m_link(k, sign, piece).start()

    to_mate(waiting[-1]).wait_recv()
    far = H

    def wide(slot):
        return pl.ds(pl.multiple_of(turn(y + slot) * 2 * F, 2 * F), 2 * F)

    cols = wide(waiting[-1])
    wg, wu = r.v_eg[:, cols], r.v_eu[:, cols]
    for piece in (3, 2, 1, 0):
        part = pieces[piece]
        lhs = r.ag[waiting[-1], part, :]
        a = r.gate[part, :] + dot(lhs, wg, 1, 1)
        b = r.up[part, :] + dot(lhs, wu, 1, 1)
        hidden = (silu(a) * b).astype(BF)
        r.hidden[part, :] = hidden
        r.m_full[far, part, :] = dot(hidden, r.v_ed[:, wide(far)]).astype(BF)
        m_mate(far, piece).start()
    for piece in (3, 2, 1, 0):
        m_mate(far, piece).wait_recv()
        m_step(H, 1, piece)
        if piece == 3:
            produce(turn(-(H - 1) * way))
    produce(turn((H - 1) * way))
    if H > 1:
        m_mate(turn(-(H - 1) * way), None).wait_recv()
        for piece in (3, 2, 1, 0):
            m_step(H - 1, -1, piece)
    if H > 2:
        for slot in (turn(-(H - 2) * way), turn((H - 2) * way)):
            produce(slot)
    for k in range(H - 1, 0, -1):
        m_mate(turn(k * way), None).wait_recv()
        for piece in (3, 2, 1, 0):
            m_step(k, 1, piece)
            if k > 1:
                if piece == 3:
                    m_mate(turn(-(k - 1) * way), None).wait_recv()
                m_step(k - 1, -1, piece)
        if k > 2:
            for slot in (turn(-(k - 2) * way), turn((k - 2) * way)):
                produce(slot)
        elif k == 2 or H == 2:
            produce(0)
        if k == g.C_AT and len(steps) > 1:
            c_both(steps.pop(0))

    m_mate(0, None).wait_recv()
    for piece in (3, 2, 1, 0):
        part = pieces[piece]
        total = pair_sum(0, piece)
        for sign in (1, -1):
            m_link(1, sign, piece).wait_recv()
            total = total + r.m_got[hop(1, sign), part, :].astype(F32)
        r.back[part, :] = total.astype(BF)
        if piece == 3:
            r.rows_ext[...] = total[M - cuts[3] :]
            for b in range(EX):
                r.back_ext[b] = r.rows_ext[b * EXT : (b + 1) * EXT, :].astype(BF)
        for b in range(EX * (piece + 1) // 4 - 1, max(EX * piece // 4, 1) - 1, -1):
            remote(
                r.back.at[pl.ds(b * MAIN, MAIN), :], r.home.at[pl.ds(opposite(b) * MAIN, MAIN), :],
                r.out_sem.at[6], r.home_sem.at[0], peer(b),
            ).start()
        if piece == 3:
            for b in range(EX - 1, 0, -1):
                remote(
                    r.back_ext.at[b], r.home_ext.at[opposite(b)],
                    r.out_sem.at[7], r.home_sem.at[1], peer(b),
                ).start()
    r.home[0:MAIN, :] = r.back[0:MAIN, :]
    r.home_ext[0] = r.back_ext[0]

    while steps:
        c_both(steps.pop(0))
    total = c_sum(0)
    for sign in (1, -1):
        c_link(1, sign).wait_recv()
        total = total + r.c_got[hop(1, sign)].astype(F32)
    r.conv_out[...] = jnp.transpose(total).astype(BF)

    bulk(r.home_ext.at[pl.ds(1, EX - 1)], r.home_sem.at[1]).wait()
    for b in range(EX):
        r.rows_ext[b * EXT : (b + 1) * EXT, :] = r.home_ext[b].astype(F32)
    r.home[M:S, :] = r.rows_ext[...].astype(BF)
    bulk(r.home.at[pl.ds(MAIN, M - MAIN), :], r.home_sem.at[0]).wait()
    result = dot(r.w_hi[...], r.home[...], 0, 0) + dot(r.w_lo[...], r.home[...], 0, 0)
    r.moe_out[...] = result.astype(BF)

    bulk(r.send_main.at[0, pl.ds(MAIN, M - MAIN), :], r.out_sem.at[0]).wait()
    bulk(r.send_ext.at[0, pl.ds(1, EX - 1)], r.out_sem.at[1]).wait()
    if DN:
        bulk(r.send_main.at[pl.ds(1, DN), pl.ds(MAIN, M - MAIN), :], r.out_sem.at[2]).wait()
        bulk(r.send_ext.at[pl.ds(1, DN), pl.ds(1, EX - 1)], r.out_sem.at[3]).wait()
    halo.wait_send()
    bulk(r.stats.at[pl.ds(1, NT - 1)], r.out_sem.at[5]).wait()
    bulk(r.back.at[pl.ds(MAIN, M - MAIN), :], r.out_sem.at[6]).wait()
    bulk(r.back_ext.at[pl.ds(1, EX - 1)], r.out_sem.at[7]).wait()
    if LA + LB:
        bulk(r.ag.at[pl.ds(0, LA + LB), :, mine], r.out_sem.at[8]).wait()
    bulk(r.ag.at[:, :, mine], r.out_sem.at[9]).wait()
    bulk(r.c_part.at[pl.ds(0, Y)], r.out_sem.at[10]).wait()
    bulk(r.c_stage, r.out_sem.at[11]).wait()
    bulk(r.m_full.at[:, :, other], r.out_sem.at[12]).wait()
    bulk(r.m_stage, r.out_sem.at[13]).wait()


def run(Z, X, args):
    (tok_a, gain_a, vw, gw, ker, cg, ow, tok_b, gain_b, routes, logits, eg, eu, ed) = args
    EX, NT = lax.axis_size("ep"), lax.axis_size("tp")
    T, D = tok_a.shape
    R, F, HU = tok_b.shape[0], vw.shape[1], eg.shape[2]
    cap = 3 * R * routes.shape[1] // (2 * EX)
    EXT, Y, DN = cap - MAIN, NT // 2, 2
    S, M = EX * cap, EX * MAIN
    given = dict(
        tok_b=tok_b, routes=routes.T, logits=logits.T, gain_b=gain_b.reshape(NT, F),
        tok_a=tok_a, gain_a=gain_a.reshape(NT, F), vw=vw, gw=gw, ker=ker, cg=cg.reshape(1, F),
        ow=ow, eg=eg[0].T, eu=eu[0].T, ed=ed[0],
    )
    vm, dma = pltpu.VMEM, pltpu.SemaphoreType.DMA
    scratch = dict(
        {"v_" + n: vm(given[n].shape, given[n].dtype) for n in INPUTS},
        in_sem=dma((len(INPUTS),)), spread=vm((EX + 8, S), BF), code=vm((EX + 8, R), F32),
        picks=vm((S, R), BF), weight=vm((EX, R), F32), w_hi=vm((S, R), BF), w_lo=vm((S, R), BF),
        send_main=vm((DN + 1, M, F), BF), send_ext=vm((DN + 1, EX, EXT, F), BF),
        recv_ext=vm((DN + 1, EX, EXT, F), BF),
        rows_ext=vm((EX * EXT, F), F32), ag=vm((Y, S, 2 * F), BF),
        out_sem=dma((14,)), a2a_sem=dma((5,)), normed_a=vm((T, D), BF), padded=vm((T + 32, F), F32),
        tail=vm((32, F), BF), halo=vm((32, F), BF), halo_sem=dma, mixed=vm((T, F), F32),
        stats=vm((NT, 2, T), F32), stat_sem=dma,
        ag_in=dma((max(Y - 1 - DN, 1), 4)), am_in=dma((Y,)),
        c_part=vm((NT, T, F), BF), c_pair=vm((Y, T, F), BF), c_stage=vm((Y - 1, T, F), BF),
        c_got=vm((Y - 1, T, F), BF), cm_in=dma, c_in=dma((Y - 1,)),
        gate=vm((S, HU), F32), up=vm((S, HU), F32), hidden=vm((S, HU), BF),
        m_full=vm((Y, S, 2 * F), BF), m_pair=vm((Y, S, F), BF), m_stage=vm((Y - 1, S, F), BF),
        m_got=vm((Y - 1, S, F), BF), mm_in=dma((Y + 4,)), m_in=dma((Y - 1, 4)), back=vm((S, F), BF), back_ext=vm((EX, EXT, F), BF),
        home=vm((S, F), BF), home_ext=vm((EX, EXT, F), BF), home_sem=dma((2,)),
    )
    names = ["in_" + n for n in INPUTS] + ["conv_out", "moe_out"] + list(scratch)
    g = SimpleNamespace(
        names=names, Z=Z, X=X, Y=Y, F=F, EX=EX, EXT=EXT, NT=NT, T=T, R=R, D=D, S=S, CH=NT * F,
        TAPS=ker.shape[0], TILES=3, DN=DN, DIRECT_AT=max(NT // 4 - (DN + 1) // 2, 1), C_AT=1,
    )
    conv_out, moe_out = pl.pallas_call(
        functools.partial(kernel, g),
        out_shape=(pltpu.VMEM((F, T), BF), pltpu.VMEM((R, F), BF)),
        in_specs=[pl.BlockSpec(memory_space=pl.ANY)] * len(INPUTS),
        out_specs=(pl.BlockSpec(memory_space=pltpu.VMEM),) * 2,
        scratch_shapes=list(scratch.values()),
        compiler_params=pltpu.CompilerParams(
            collective_id=0, has_side_effects=True, vmem_limit_bytes=60 * 1024 * 1024
        ),
    )(*[given[n] for n in INPUTS])
    return conv_out, moe_out.T


def solution(mesh, Z=8, X=4):
    return jax.shard_map(
        lambda *args: run(Z, X, args),
        mesh=mesh,
        in_specs=(
            P("ep", None), P(), P(None, "tp"), P(None, "tp"), P(None, "tp"), P("tp"), P("tp", None),
            P("ep", None), P(), P("ep", None), P("ep", None), P("ep", None, "tp"),
            P("ep", None, "tp"), P("ep", "tp", None),
        ),
        out_specs=(P("tp", "ep"), P("tp", "ep")),
        check_vma=False,
    )
```
